32 devices in a mesh: grp: 2 (over y), sp: 4 (over z), tp: 4 (over x, core).
Axes of the slice: x: 2, y: 2, z: 4, core: 2. Of those that a mesh axis runs over, the one named last changes fastest.
Arguments:
- query_rows: bfloat16 [1024, 1024], P(('grp', 'sp'), 'tp'), parts along dimension 0, may hold values from -64 to 64
- key_rows: bfloat16 [1024, 512], P(('grp', 'sp'), 'tp'), parts along dimension 0, may hold values from -16 to 16
- value_rows: bfloat16 [1024, 512], P(('grp', 'sp'), 'tp'), parts along dimension 0, may hold values from -6 to 6
- sink_logit: float32 [16], P('tp'), may hold values from 3.5 to 7
- out_weight: bfloat16 [1024, 2048], P('tp'), may hold values from -0.1875 to 0.1875
- residual: bfloat16 [1024, 2048], P(('grp', 'sp', 'tp')), parts along dimension 0, may hold values from -6 to 6
- norm_gain: float32 [2048], replicated, may hold values from 0.1 to 1.9
- routes: int32 [1024, 6], P(('grp', 'sp', 'tp')), parts along dimension 0, may hold values from 0 to 15, as said below
- gate_weights: float32 [1024, 6], P(('grp', 'sp', 'tp')), parts along dimension 0, may hold values from 0.1 to 0.8
- expert_gate: bfloat16 [16, 2048, 512], P(('sp', 'tp')), may hold values from -0.125 to 0.125
- expert_up: bfloat16 [16, 2048, 512], P(('sp', 'tp')), may hold values from -0.125 to 0.125
- expert_down: bfloat16 [16, 512, 2048], P(('sp', 'tp')), may hold values from -0.25 to 0.25
- shared_gate: bfloat16 [2048, 512], P(None, 'tp'), may hold values from -0.125 to 0.125
- shared_up: bfloat16 [2048, 512], P(None, 'tp'), may hold values from -0.125 to 0.125
- shared_down: bfloat16 [512, 2048], P('tp'), may hold values from -0.25 to 0.25
Outputs:
- layer_out: bfloat16 [1024, 2048], P(('grp', 'sp', 'tp')), parts along dimension 0
The draws below stay inside these ranges and needn't reach their ends.
There are 2 independent parts, one for each index of `grp`. The reference program is written for one: setup_inputs(seed, part) draws one part's arguments, and reference() takes and returns one part's arrays. A program takes and returns all parts, laid end to end along the dimension named above; an argument that names none is the same for every part. Nothing has to cross between parts.
Inputs may be any that keep to these rules, and one draw needn't show every extreme that they name: `routes`: in each aligned block of 32 rows (the rows of one device) every row names 6 different experts and no expert is named by more than 24 rows; in every draw some expert is named by exactly 24 rows of every block.
All inputs are finite; a program needn't handle non-finite values.
Results may differ from the reference program's by a relative error of at most 0.015.
Values may be sent and summed in bfloat16 or wider, within the bound.
A program may use at most 64 MiB of HBM per device.

```python
import jax
import jax.numpy as jnp
from jax import lax

D = 2048
HEADS = 16
KVH = 8
HEAD = 64
WINDOW = 128
FF = 512
SHARED = 512
TOPK = 6
TOKENS = 512
ROWS = 32
EXPERTS = 16
CAP = 24
N_TP = 4


def plant_pair(key):
    query_key = jax.random.fold_in(key, 101)
    keys_key = jax.random.fold_in(key, 102)
    queries = jnp.clip(jax.random.normal(query_key, (TOKENS, HEADS * HEAD), jnp.float32), -6.0, 6.0)
    keys_all = jnp.clip(jax.random.normal(keys_key, (TOKENS, KVH * HEAD), jnp.float32), -6.0, 6.0)
    return (jnp.clip(queries, -64.0, 64.0), jnp.clip(keys_all, -16.0, 16.0))


def draw_query_rows(key, part):
    return plant_pair(key)[0].astype(jnp.bfloat16)


def draw_key_rows(key, part):
    return plant_pair(key)[1].astype(jnp.bfloat16)


def draw_residual(key, part):
    base_key = jax.random.fold_in(key, 201)
    row_key = jax.random.fold_in(key, 202)
    col_key = jax.random.fold_in(key, 203)
    base_draw = jnp.clip(jax.random.normal(base_key, (TOKENS, D), jnp.float32), -3.5, 3.5)
    row_scale = jnp.exp(jax.random.uniform(row_key, (TOKENS, 1), jnp.float32, jnp.log(0.4), jnp.log(4.0)))
    col_scale = jnp.exp(jax.random.uniform(col_key, (1, D), jnp.float32, jnp.log(0.4), jnp.log(4.0)))
    return (0.1 * base_draw * row_scale * col_scale).astype(jnp.bfloat16)


def draw_routes(key, part):
    block_count = TOKENS // ROWS
    special = jax.random.randint(jax.random.fold_in(key, 7), (), 0, EXPERTS)
    smallest = (CAP + 1) // 2

    def one_block(block_key):
        size_key, perm_key, row_key = jax.random.split(block_key, 3)
        group_size = jax.random.randint(size_key, (EXPERTS,), smallest, CAP + 1).at[0].set(CAP)
        group_end = jnp.cumsum(group_size)
        slot_index = jnp.arange(ROWS * TOPK, dtype=jnp.int32)
        group_of = jnp.sum((group_end[None, :] <= slot_index[:, None]).astype(jnp.int32), axis=1)
        others = jax.random.permutation(perm_key, EXPERTS - 1).astype(jnp.int32) + 1
        mapping = (jnp.concatenate([jnp.zeros((1,), jnp.int32), others]) + special) % EXPERTS
        chosen = mapping[group_of].reshape(TOPK, ROWS).T
        return chosen[jax.random.permutation(row_key, ROWS)]
    blocks_out = jax.vmap(one_block)(jax.random.split(jax.random.fold_in(key, 9), block_count))
    return blocks_out.reshape(TOKENS, TOPK).astype(jnp.int32)


def shard_levels(stream_key, extent, shards, least, top_value):
    def one(axis_at, shards_of):
        draws = jax.random.uniform(jax.random.fold_in(jax.random.fold_in(stream_key, 6), axis_at), (shards_of,), jnp.float32, least / len(shards), top_value / len(shards))
        return jnp.repeat(jnp.exp(draws), extent[axis_at] // shards_of).reshape((-1,) + (1,) * (len(extent) - axis_at - 1))

    level = one(*shards[0])
    for cut in shards[1:]:
        level = level * one(*cut)
    return level


def noise(own_key, dims, scale, reach, shards=(), held_as=jnp.bfloat16):
    array = jax.random.normal(own_key, dims, jnp.float32) * scale
    if len(shards) > 0:
        array = shard_levels(own_key, dims, shards, -0.22, 0.18) * array
    return jnp.clip(array, min=-reach, max=reach).astype(held_as)


def setup_inputs(seed: int = 0, part: int = 0) -> dict:
    streams_of = jax.random.split(jax.random.key(seed), 16)
    part_keys = jax.random.split(jax.random.fold_in(streams_of[15], part), 16)
    query_rows = draw_query_rows(jax.random.fold_in(jax.random.fold_in(streams_of[15], part), 71), part)
    key_rows = draw_key_rows(jax.random.fold_in(jax.random.fold_in(streams_of[15], part), 71), part)
    value_rows = noise(part_keys[2], (TOKENS, KVH * HEAD), 1.0, 6.0, ((0, 4), (1, 4)))
    sink_logit = jnp.clip(3.5 + 3.5 * jax.random.uniform(streams_of[3], (HEADS,), jnp.float32) ** shard_levels(streams_of[3], (HEADS,), ((0, 4),), -0.2, 0.2), 3.5, 7.0)
    out_weight = noise(streams_of[4], (HEADS * HEAD, D), (HEADS * HEAD) ** -0.5, 0.1875, ((0, 4),))
    residual = draw_residual(jax.random.fold_in(jax.random.fold_in(streams_of[15], part), 71), part)
    norm_gain = jnp.clip(1.0 + 0.18 * jax.random.normal(streams_of[6], (D,), jnp.float32), 0.1, 1.9)
    routes = draw_routes(jax.random.fold_in(jax.random.fold_in(streams_of[15], part), 71), part)
    gate_weights = jnp.clip(0.1 + 0.7 * jax.random.uniform(part_keys[8], (TOKENS, TOPK), jnp.float32) ** shard_levels(part_keys[8], (TOKENS, TOPK), ((0, 16),), -0.2, 0.2), 0.1, 0.8)
    expert_gate = noise(streams_of[9], (EXPERTS, D, FF), D ** -0.5, 0.125, ((0, 16),))
    expert_up = noise(streams_of[10], (EXPERTS, D, FF), D ** -0.5, 0.125, ((0, 16),))
    expert_down = noise(streams_of[11], (EXPERTS, FF, D), FF ** -0.5, 0.25, ((0, 16),))
    shared_gate = noise(streams_of[12], (D, SHARED), D ** -0.5, 0.125, ((1, 4),))
    shared_up = noise(streams_of[13], (D, SHARED), D ** -0.5, 0.125, ((1, 4),))
    shared_down = noise(streams_of[14], (SHARED, D), SHARED ** -0.5, 0.25, ((0, 4),))
    return {"query_rows": query_rows, "key_rows": key_rows, "value_rows": value_rows, "sink_logit": sink_logit, "out_weight": out_weight, "residual": residual, "norm_gain": norm_gain, "routes": routes, "gate_weights": gate_weights, "expert_gate": expert_gate, "expert_up": expert_up, "expert_down": expert_down, "shared_gate": shared_gate, "shared_up": shared_up, "shared_down": shared_down}


norm_eps = 1e-06

def band_view(tensor, blocks):
    shaped = tensor.reshape(blocks, WINDOW, tensor.shape[1], tensor.shape[2])
    padded = jnp.pad(shaped, ((1, 1), (0, 0), (0, 0), (0, 0)))
    return jnp.concatenate([padded[:-2], padded[1:-1], padded[2:]], axis=1)

def attention(query_rows, key_rows, value_rows, sink_logit):
    length = query_rows.shape[0]
    blocks = length // WINDOW
    groups = HEADS // KVH
    queries = query_rows.astype(jnp.float32).reshape(blocks, WINDOW, KVH, groups, HEAD)
    keyband = band_view(key_rows.astype(jnp.float32).reshape(length, KVH, HEAD), blocks)
    valband = band_view(value_rows.astype(jnp.float32).reshape(length, KVH, HEAD), blocks)
    block_ids = jnp.arange(blocks, dtype=jnp.int32)[:, None, None]
    query_pos = block_ids * WINDOW + jnp.arange(WINDOW, dtype=jnp.int32)[None, :, None]
    key_pos = (block_ids - 1) * WINDOW + jnp.arange(3 * WINDOW, dtype=jnp.int32)[None, None, :]
    in_window = (jnp.abs(key_pos - query_pos) <= WINDOW) & (key_pos >= 0) & (key_pos < length)

    def one_head(head_index):
        query_part = queries[:, :, head_index]
        key_part = keyband[:, :, head_index]
        value_part = valband[:, :, head_index]
        scores = jnp.einsum('nqgd,nkd->ngqk', query_part, key_part) * HEAD ** (-0.5)
        scores = jnp.where(in_window[:, None], scores, -jnp.inf)
        sink_part = lax.dynamic_slice_in_dim(sink_logit, head_index * groups, groups).reshape(1, groups, 1, 1)
        row_max = jnp.maximum(sink_part, lax.optimization_barrier(jnp.max(scores, axis=-1, keepdims=True)))
        shifted = jnp.exp(scores - row_max)
        denominator = jnp.exp(sink_part - row_max) + lax.optimization_barrier(jnp.sum(shifted, axis=-1, keepdims=True))
        weights = lax.optimization_barrier((shifted / denominator).astype(jnp.bfloat16))
        weighted = jnp.einsum('ngqk,nkd->nqgd', weights.astype(jnp.float32), value_part)
        return weighted.astype(jnp.bfloat16)
    heads_out = lax.map(one_head, jnp.arange(KVH, dtype=jnp.int32))
    return jnp.transpose(heads_out, (1, 2, 0, 3, 4)).reshape(length, HEADS * HEAD)

def routed_experts(normed, routes, gate_weights, expert_gate, expert_up, expert_down):
    tokens = normed.shape[0]
    model_width = normed.shape[1]
    copies = tokens * TOPK
    block_rows = 64
    flat_expert = routes.reshape(-1).astype(jnp.int32)
    order_index = jnp.argsort(flat_expert, stable=True).astype(jnp.int32)
    sorted_expert = flat_expert[order_index]
    counts = jax.ops.segment_sum(jnp.ones((copies,), jnp.int32), flat_expert, num_segments=EXPERTS)
    padded_counts = (counts + block_rows - 1) // block_rows * block_rows
    padded_end = jnp.cumsum(padded_counts).astype(jnp.int32)
    padded_start = padded_end - padded_counts
    group_start = (jnp.cumsum(counts) - counts).astype(jnp.int32)
    target = padded_start[sorted_expert] + jnp.arange(copies, dtype=jnp.int32) - group_start[sorted_expert]
    block_count = (copies + EXPERTS * (block_rows - 1) + block_rows - 1) // block_rows
    slot_copy = jnp.full((block_count * block_rows,), copies, jnp.int32).at[target].set(order_index)
    block_first = jnp.arange(block_count, dtype=jnp.int32) * block_rows
    block_expert = jnp.minimum(jnp.searchsorted(padded_end, block_first, side='right'), EXPERTS - 1).astype(jnp.int32)
    copy_token = jnp.concatenate([jnp.arange(copies, dtype=jnp.int32) // TOPK, jnp.full((1,), tokens, jnp.int32)])
    padded_rows = jnp.concatenate([normed, jnp.zeros((1, model_width), normed.dtype)], axis=0)

    def run_block(inputs):
        slot_ids, expert_id = inputs
        block_in = padded_rows[copy_token[slot_ids]]
        gate_part = jnp.dot(block_in, expert_gate[expert_id], preferred_element_type=jnp.float32)
        up_part = jnp.dot(block_in, expert_up[expert_id], preferred_element_type=jnp.float32)
        hidden = (jax.nn.silu(gate_part) * up_part).astype(jnp.bfloat16)
        return jnp.dot(hidden, expert_down[expert_id], preferred_element_type=jnp.float32).astype(jnp.bfloat16)
    outputs = lax.map(run_block, (slot_copy.reshape(block_count, block_rows), block_expert))
    per_copy = jnp.zeros((copies + 1, model_width), jnp.bfloat16).at[slot_copy].set(outputs.reshape(-1, model_width))
    per_copy = lax.optimization_barrier(per_copy[:copies].reshape(tokens, TOPK, model_width))
    return lax.optimization_barrier(jnp.sum(gate_weights[:, :, None] * per_copy.astype(jnp.float32), axis=1))

def shared_expert(normed, shared_gate, shared_up, shared_down):
    gate_part = jnp.dot(normed, shared_gate, preferred_element_type=jnp.float32)
    up_part = jnp.dot(normed, shared_up, preferred_element_type=jnp.float32)
    hidden = (jax.nn.silu(gate_part) * up_part).astype(jnp.bfloat16)
    unit_count = SHARED // N_TP
    totals = jnp.zeros((normed.shape[0], shared_down.shape[1]), jnp.float32)
    for group_index in range(N_TP):
        lower_unit = group_index * unit_count
        partial_sum = jnp.dot(hidden[:, lower_unit:lower_unit + unit_count], shared_down[lower_unit:lower_unit + unit_count], preferred_element_type=jnp.float32)
        totals = totals + lax.optimization_barrier(partial_sum.astype(jnp.bfloat16)).astype(jnp.float32)
    return totals

def reference(query_rows, key_rows, value_rows, sink_logit, out_weight, residual, norm_gain, routes, gate_weights, expert_gate, expert_up, expert_down, shared_gate, shared_up, shared_down):
    attended = attention(query_rows, key_rows, value_rows, sink_logit)
    projected = jnp.dot(attended, out_weight, preferred_element_type=jnp.float32)
    stream = residual.astype(jnp.float32) + projected
    normed = (stream * lax.rsqrt(lax.optimization_barrier(jnp.mean(stream * stream, axis=-1, keepdims=True)) + norm_eps) * norm_gain).astype(jnp.bfloat16)
    routed = routed_experts(normed, routes, gate_weights, expert_gate, expert_up, expert_down)
    shared = shared_expert(normed, shared_gate, shared_up, shared_down)
    return (stream + routed + shared).astype(jnp.bfloat16)
```

```python
import functools

import jax
import jax.numpy as jnp
from jax import lax
from jax.experimental import pallas as pl
from jax.experimental.pallas import tpu as pltpu
from jax.sharding import PartitionSpec as P

HEAD = 64
WINDOW = 128
TOPK = 6


norm_eps = 1e-06


def with_halo(block, sides, width):
    for axis, dim in sides:
        count = lax.axis_size(axis)
        forward = [(i, i + 1) for i in range(count - 1)]
        backward = [(target, source) for source, target in forward]
        low = lax.ppermute(
            lax.slice_in_dim(block, block.shape[dim] - width, None, axis=dim), axis, forward
        )
        high = lax.ppermute(lax.slice_in_dim(block, 0, width, axis=dim), axis, backward)
        block = jnp.concatenate([low, block, high], axis=dim)
    return block


def window_attention(query_rows, key_rows, value_rows, sink_logit):
    local_len = query_rows.shape[0]
    head_size = HEAD
    local_kv = key_rows.shape[1] // head_size
    local_heads = query_rows.shape[1] // head_size
    grouped = local_heads // local_kv
    blocks = local_len // WINDOW
    stacked = jnp.stack([key_rows, value_rows])
    widened = with_halo(stacked, (("sp", 1),), WINDOW)
    banded = widened.reshape(2, blocks + 2, WINDOW, local_kv, head_size)
    banded = jnp.concatenate([banded[:, :-2], banded[:, 1:-1], banded[:, 2:]], axis=2)
    queries = query_rows.reshape(blocks, WINDOW, local_kv, grouped, head_size)
    scores = jnp.einsum(
        "nqhgd,nkhd->nhgqk", queries, banded[0], preferred_element_type=jnp.float32
    ) * head_size ** (-0.5)
    seq_start = lax.axis_index("sp") * local_len
    total_len = lax.axis_size("sp") * local_len
    block_ids = jnp.arange(blocks, dtype=jnp.int32)[:, None, None]
    query_pos = seq_start + block_ids * WINDOW + jnp.arange(WINDOW, dtype=jnp.int32)[None, :, None]
    key_pos = (
        seq_start
        + (block_ids - 1) * WINDOW
        + jnp.arange(3 * WINDOW, dtype=jnp.int32)[None, None, :]
    )
    in_window = (jnp.abs(key_pos - query_pos) <= WINDOW) & (key_pos >= 0) & (key_pos < total_len)
    scores = jnp.where(in_window[:, None, None], scores, -jnp.inf)
    sink_part = sink_logit.reshape(1, local_kv, grouped, 1, 1)
    row_max = jnp.maximum(sink_part, jnp.max(scores, axis=-1, keepdims=True))
    shifted = jnp.exp(scores - row_max)
    denominator = jnp.exp(sink_part - row_max) + jnp.sum(shifted, axis=-1, keepdims=True)
    weights = (shifted / denominator).astype(jnp.bfloat16)
    attended = jnp.einsum(
        "nhgqk,nkhd->nqhgd", weights, banded[1], preferred_element_type=jnp.float32
    )
    return attended.astype(jnp.bfloat16).reshape(local_len, local_heads * head_size)


def body(
    query_rows,
    key_rows,
    value_rows,
    sink_logit,
    out_weight,
    residual,
    norm_gain,
    routes,
    gate_weights,
    expert_gate,
    expert_up,
    expert_down,
    shared_gate,
    shared_up,
    shared_down,
):
    attended = window_attention(query_rows, key_rows, value_rows, sink_logit)
    tok_dev = attended.shape[0]
    tok_rows = residual.shape[0]
    model_width = residual.shape[1]
    projected = lax.psum_scatter(
        jnp.dot(attended, out_weight, preferred_element_type=jnp.float32).astype(jnp.bfloat16),
        "tp",
        scatter_dimension=0,
        tiled=True,
    ).astype(jnp.float32)
    stream = residual.astype(jnp.float32) + projected
    normed = (
        stream * lax.rsqrt(jnp.mean(stream * stream, axis=-1, keepdims=True) + norm_eps) * norm_gain
    ).astype(jnp.bfloat16)
    sp_count = lax.axis_size("sp")
    tp_count = lax.axis_size("tp")
    experts_all = sp_count * tp_count
    capacity = (2 * tok_dev * TOPK + tp_count * experts_all - 1) // (tp_count * experts_all)
    copies = tok_rows * TOPK
    flat_expert = routes.reshape(-1)
    one_hot = (flat_expert[:, None] == jnp.arange(experts_all, dtype=jnp.int32)[None, :]).astype(
        jnp.int32
    )
    rank_in_expert = jnp.sum(jnp.cumsum(one_hot, axis=0) * one_hot, axis=1) - 1
    target_slot = flat_expert * capacity + rank_in_expert
    slot_token = (
        jnp.full((experts_all * capacity,), tok_rows, jnp.int32)
        .at[target_slot]
        .set(jnp.arange(copies, dtype=jnp.int32) // TOPK)
    )
    padded_rows = jnp.concatenate([normed, jnp.zeros((1, model_width), jnp.bfloat16)], axis=0)
    outgoing = padded_rows[slot_token].reshape(experts_all, capacity, model_width)
    incoming = lax.all_to_all(outgoing, ("sp", "tp"), split_axis=0, concat_axis=0, tiled=True)
    shaped = incoming.reshape(-1, model_width)
    gate_part = jnp.dot(shaped, expert_gate[0], preferred_element_type=jnp.float32)
    up_part = jnp.dot(shaped, expert_up[0], preferred_element_type=jnp.float32)
    hidden = (jax.nn.silu(gate_part) * up_part).astype(jnp.bfloat16)
    result = jnp.dot(hidden, expert_down[0], preferred_element_type=jnp.float32).astype(
        jnp.bfloat16
    )
    returned = lax.all_to_all(
        result.reshape(incoming.shape), ("sp", "tp"), split_axis=0, concat_axis=0, tiled=True
    )
    returned = returned.reshape(experts_all * capacity, model_width)
    gathered_copies = returned[target_slot].reshape(tok_rows, TOPK, model_width)
    routed = jnp.sum(gate_weights[:, :, None] * gathered_copies.astype(jnp.float32), axis=1)
    slab_rows = lax.all_gather(normed, "tp", axis=0, tiled=True)
    gate_part = jnp.dot(slab_rows, shared_gate, preferred_element_type=jnp.float32)
    up_part = jnp.dot(slab_rows, shared_up, preferred_element_type=jnp.float32)
    hidden = (jax.nn.silu(gate_part) * up_part).astype(jnp.bfloat16)
    partials = jnp.dot(hidden, shared_down, preferred_element_type=jnp.float32)
    shared = lax.psum_scatter(
        partials.astype(jnp.bfloat16), "tp", scatter_dimension=0, tiled=True
    ).astype(jnp.float32)
    return (stream + routed + shared).astype(jnp.bfloat16)


VMEM_BYTES = 66 * 1000 * 1000
PAIR = 2
LANES = 128
CHUNKS = 2


def fused_kernel(
    sp,
    tp,
    q_hbm,
    k_hbm,
    v_hbm,
    sink_ref,
    wo_hbm,
    res_hbm,
    gain_hbm,
    routes_hbm,
    gw_hbm,
    eg_hbm,
    eu_hbm,
    ed_hbm,
    sg_hbm,
    su_hbm,
    sd_hbm,
    out_ref,
    q_v,
    k_v,
    v_v,
    wo_v,
    res_v,
    gain_v,
    routes_v,
    gw_v,
    eg_v,
    eu_v,
    ed_v,
    sg_v,
    su_v,
    sd_v,
    halo_k,
    halo_v,
    att_v,
    proj,
    psend,
    precv,
    pxs,
    pxr,
    stream_v,
    nrm,
    part,
    crecv,
    xsend,
    xrecv,
    zsend,
    zrecv,
    load_sem,
    halo_s,
    halo_r,
    ps_sem,
    pr_sem,
    s_core,
    s_x,
    s_up,
    s_dn,
    nrm_r,
    cs_sem,
    cr_sem,
    xs_sem,
    xr_sem,
    zs_sem,
    zr_sem,
):
    z = lax.axis_index("sp")
    t = lax.axis_index("tp")
    c = t % PAIR
    x = t // PAIR
    t_core = x * PAIR + (1 - c)
    t_x = (1 - x) * PAIR + c
    t_far = (1 - x) * PAIR + (1 - c)
    core = {"tp": t_core}
    xnbr = {"tp": t_x}

    def at_z(pos):
        return {"sp": pos}

    def rcopy(src, dst, ssem, rsem, dev):
        return pltpu.make_async_remote_copy(
            src_ref=src,
            dst_ref=dst,
            send_sem=ssem,
            recv_sem=rsem,
            device_id=dev,
            device_id_type=pl.DeviceIdType.MESH,
        )

    moves = [
        (k_hbm, k_v),
        (v_hbm, v_v),
        (q_hbm, q_v),
        (wo_hbm, wo_v),
        (res_hbm, res_v),
        (gain_hbm, gain_v),
        (routes_hbm, routes_v),
        (gw_hbm, gw_v),
        (sg_hbm, sg_v),
        (su_hbm, su_v),
        (sd_hbm, sd_v),
        (eg_hbm.at[0], eg_v),
        (eu_hbm.at[0], eu_v),
        (ed_hbm.at[0], ed_v),
    ]
    loads = [pltpu.make_async_copy(a, b, load_sem.at[i]) for i, (a, b) in enumerate(moves)]
    barrier = pltpu.get_barrier_semaphore()
    for dev in (core, xnbr):
        pl.semaphore_signal(barrier, inc=1, device_id=dev, device_id_type=pl.DeviceIdType.MESH)
    @pl.when(z > 0)
    def _():
        pl.semaphore_signal(
            barrier, inc=1, device_id=at_z(z - 1), device_id_type=pl.DeviceIdType.MESH
        )

    @pl.when(z < sp - 1)
    def _():
        pl.semaphore_signal(
            barrier, inc=1, device_id=at_z(z + 1), device_id_type=pl.DeviceIdType.MESH
        )

    for load in loads:
        load.start()
    rows = stream_v.shape[0]
    width = stream_v.shape[1]
    length = q_v.shape[0]
    heads = q_v.shape[1] // HEAD
    grouped = heads // (k_v.shape[1] // HEAD)

    @pl.when(z == 0)
    def _():
        halo_k[0] = jnp.zeros(halo_k.shape[1:], halo_k.dtype)
        halo_v[0] = jnp.zeros(halo_v.shape[1:], halo_v.dtype)

    @pl.when(z == sp - 1)
    def _():
        halo_k[1] = jnp.zeros(halo_k.shape[1:], halo_k.dtype)
        halo_v[1] = jnp.zeros(halo_v.shape[1:], halo_v.dtype)

    loads[0].wait()
    loads[1].wait()
    peers = 2 + jnp.where(z > 0, 1, 0) + jnp.where(z < sp - 1, 1, 0)
    pl.semaphore_wait(barrier, peers)

    def halo(up):
        pos = z + 1 if up else z - 1
        slot = 0 if up else 1
        row = 0 if up else 1
        return (
            rcopy(k_v, halo_k.at[slot], halo_s.at[row, 0], halo_r.at[slot, 0], at_z(pos)),
            rcopy(v_v, halo_v.at[slot], halo_s.at[row, 1], halo_r.at[slot, 1], at_z(pos)),
        )

    @pl.when(z < sp - 1)
    def _():
        for copy in halo(True):
            copy.start()

    @pl.when(z > 0)
    def _():
        for copy in halo(False):
            copy.start()

    loads[6].wait()
    loads[7].wait()
    half = LANES // 2
    lane = lax.broadcasted_iota(jnp.int32, (rows, LANES), 1)
    unit = lax.broadcasted_iota(jnp.int32, (LANES, rows), 0)
    unit = jnp.where(unit < half, unit, unit - half)
    combine = jnp.zeros((LANES, rows), jnp.float32)
    for k in range(TOPK):
        combine = combine + jnp.where(routes_v[k : k + 1] == unit, gw_v[k : k + 1], 0.0)
    combine = combine.T
    high = combine.astype(jnp.bfloat16)
    low = (combine - high.astype(jnp.float32)).astype(jnp.bfloat16)
    nrm[z, t, :, width:] = jnp.where(
        lane < half, high.astype(jnp.float32), low.astype(jnp.float32)
    ).astype(jnp.bfloat16)

    loads[2].wait()
    contract = (((1,), (1,)), ((), ()))
    scale = HEAD ** (-0.5)

    def cols(head):
        return slice(head * HEAD, (head + 1) * HEAD)

    own_scores = []
    for head in range(heads):
        own_scores.append(
            lax.dot_general(
                q_v[:, cols(head)],
                k_v[:, cols(head // grouped)],
                contract,
                preferred_element_type=jnp.float32,
            )
            * scale
        )

    @pl.when(z > 0)
    def _():
        for copy in (
            rcopy(k_v, halo_k.at[0], halo_s.at[0, 0], halo_r.at[0, 0], core),
            rcopy(v_v, halo_v.at[0], halo_s.at[0, 1], halo_r.at[0, 1], core),
        ):
            copy.wait_recv()

    @pl.when(z < sp - 1)
    def _():
        for copy in (
            rcopy(k_v, halo_k.at[1], halo_s.at[1, 0], halo_r.at[1, 0], core),
            rcopy(v_v, halo_v.at[1], halo_s.at[1, 1], halo_r.at[1, 1], core),
        ):
            copy.wait_recv()

    qi = lax.broadcasted_iota(jnp.int32, (length, length), 0)
    ki = lax.broadcasted_iota(jnp.int32, (length, length), 1)
    low_bound = jnp.where(z > 0, 0, length)
    high_bound = jnp.where(z < sp - 1, 0, length)
    low_mask = ki - qi >= low_bound
    high_mask = qi - ki >= high_bound
    for head in range(heads):
        kv = cols(head // grouped)
        qh = q_v[:, cols(head)]
        s_own = own_scores[head]
        s_low = jnp.where(
            low_mask,
            lax.dot_general(qh, halo_k[0, :, kv], contract, preferred_element_type=jnp.float32)
            * scale,
            -jnp.inf,
        )
        s_high = jnp.where(
            high_mask,
            lax.dot_general(qh, halo_k[1, :, kv], contract, preferred_element_type=jnp.float32)
            * scale,
            -jnp.inf,
        )
        sink = sink_ref[head]
        top = jnp.max(
            jnp.maximum(jnp.maximum(s_low, s_high), s_own), axis=-1, keepdims=True
        )
        top = jnp.maximum(top, sink)
        e_low = jnp.exp(s_low - top)
        e_own = jnp.exp(s_own - top)
        e_high = jnp.exp(s_high - top)
        denominator = jnp.exp(sink - top) + jnp.sum(e_low + e_own + e_high, axis=-1, keepdims=True)
        inverse = 1.0 / denominator
        attended = jnp.dot(
            (e_own * inverse).astype(jnp.bfloat16), v_v[:, kv], preferred_element_type=jnp.float32
        )
        attended += jnp.dot(
            (e_low * inverse).astype(jnp.bfloat16),
            halo_v[0, :, kv],
            preferred_element_type=jnp.float32,
        )
        attended += jnp.dot(
            (e_high * inverse).astype(jnp.bfloat16),
            halo_v[1, :, kv],
            preferred_element_type=jnp.float32,
        )
        att_v[:, cols(head)] = attended.astype(jnp.bfloat16)

    loads[3].wait()
    proj[...] = jnp.dot(
        att_v[...], wo_v[...], preferred_element_type=jnp.float32
    ).reshape(proj.shape)
    piece = rows // CHUNKS

    def cut(j):
        return pl.ds(j * piece, piece)

    pcore = []
    for order, xx in enumerate((1 - x, x)):
        psend[xx] = proj[xx * PAIR + (1 - c)].astype(jnp.bfloat16)
        pcore.append(rcopy(psend.at[xx], precv.at[xx], ps_sem.at[order], pr_sem.at[order], core))
        pcore[-1].start()
    pcore[0].wait_recv()
    pcross = []
    for j in range(CHUNKS):
        pxs[cut(j)] = (proj[t_x, cut(j)] + precv[1 - x, cut(j)].astype(jnp.float32)).astype(
            jnp.bfloat16
        )
        pcross.append(
            rcopy(
                pxs.at[cut(j)], pxr.at[cut(j)], ps_sem.at[PAIR + j], pr_sem.at[PAIR + j], xnbr
            )
        )
        pcross[-1].start()
    loads[4].wait()
    loads[5].wait()
    pcore[1].wait_recv()
    stream_v[...] = res_v[...].astype(jnp.float32) + proj[t] + precv[x].astype(jnp.float32)

    def carry(g, tt, j, ssem, dev):
        ref = nrm.at[g, tt, cut(j)]
        return rcopy(ref, ref, ssem, nrm_r.at[g, tt, j], dev)

    def to_core(g, tt, j):
        return carry(g, tt, j, s_core.at[g, tt, j], core)

    def to_x(g, j):
        return carry(g, t, j, s_x.at[g, j], xnbr)

    def to_up(g, j):
        return carry(g, t, j, s_up.at[g, j], at_z(z + 1))

    def to_dn(g, j):
        return carry(g, t, j, s_dn.at[g, j], at_z(z - 1))

    def nrm_wait(g, tt, j):
        to_core(g, tt, j).wait_recv()

    below = z
    above = sp - 1 - z
    short = jnp.minimum(below, above)

    def group_of(i):
        if i < 0:
            return z
        paired = i < 2 * short
        dist = jnp.where(paired, i // 2 + 1, i - short + 1)
        if i % 2 == 0:
            sign_pair = -1
        else:
            sign_pair = 1
        sign = jnp.where(paired, sign_pair, jnp.where(below > above, -1, 1))
        return z + sign * dist

    groups = {i: group_of(i) for i in range(-1, sp - 1)}

    def stage_a(i, j):
        g = groups[i]
        if i >= 0:
            nrm_wait(g, t, j)

        @pl.when((g <= z) & (z < sp - 1))
        def _():
            to_up(g, j).start()

        @pl.when((g >= z) & (z > 0))
        def _():
            to_dn(g, j).start()

        to_x(g, j).start()
        to_core(g, t, j).start()

    def stage_b(i, j):
        g = groups[i]
        nrm_wait(g, t_x, j)
        to_core(g, t_x, j).start()

    def stage_c(i):
        g = groups[i]
        for j in range(CHUNKS):
            nrm_wait(g, t_core, j)
            nrm_wait(g, t_far, j)

    expert = z * tp + t

    def part_send(g):
        return rcopy(part.at[g, 1 - c], crecv.at[g], cs_sem.at[g], cr_sem.at[g], core)

    def cross_send(g, j):
        return rcopy(
            xsend.at[g, cut(j)], xrecv.at[g, cut(j)], xs_sem.at[g, j], xr_sem.at[g, j], xnbr
        )

    def line_send(g, j):
        return rcopy(
            zsend.at[g, cut(j)], zrecv.at[z, cut(j)], zs_sem.at[g, j], zr_sem.at[z, j], at_z(g)
        )

    def silu(v):
        return v / (1.0 + jnp.exp(-v))

    def stage_d(i):
        g = groups[i]
        if i < 0:
            for k in range(8, 14):
                loads[k].wait()
        block = nrm[g].reshape(tp * rows, nrm.shape[-1])
        acts = block[:, :width]
        tail = block[:, width:].astype(jnp.float32)
        lanes = lax.broadcasted_iota(jnp.int32, tail.shape, 1)
        mine = (lanes == expert) | (lanes == expert + half)
        weight = jnp.sum(jnp.where(mine, tail, 0.0), axis=-1, keepdims=True)
        gate = jnp.dot(acts, eg_v[...], preferred_element_type=jnp.float32)
        up = jnp.dot(acts, eu_v[...], preferred_element_type=jnp.float32)
        hidden = (silu(gate) * up).astype(jnp.bfloat16)
        result = jnp.dot(hidden, ed_v[...], preferred_element_type=jnp.float32)
        result = weight * result.astype(jnp.bfloat16).astype(jnp.float32)
        if i < 0:
            gate = jnp.dot(acts, sg_v[...], preferred_element_type=jnp.float32)
            up = jnp.dot(acts, su_v[...], preferred_element_type=jnp.float32)
            hidden = (silu(gate) * up).astype(jnp.bfloat16)
            shared = jnp.dot(hidden, sd_v[...], preferred_element_type=jnp.float32)
            result = result + shared.astype(jnp.bfloat16).astype(jnp.float32)
        result = result.astype(jnp.bfloat16)
        for tt in range(tp):
            part[g, tt % PAIR, tt // PAIR] = result[tt * rows : (tt + 1) * rows]
        part_send(g).start()

    def stage_e(i):
        g = groups[i]
        part_send(g).wait_recv()
        for j in range(CHUNKS):
            xsend[g, cut(j)] = (
                part[g, c, 1 - x, cut(j)].astype(jnp.float32)
                + crecv[g, 1 - x, cut(j)].astype(jnp.float32)
            ).astype(jnp.bfloat16)
            cross_send(g, j).start()

    def column(g, j):
        cross_send(g, j).wait_recv()
        return (
            part[g, c, x, cut(j)].astype(jnp.float32)
            + crecv[g, x, cut(j)].astype(jnp.float32)
            + xrecv[g, cut(j)].astype(jnp.float32)
        )

    def stage_f(i):
        g = groups[i]
        for j in range(CHUNKS):
            zsend[g, cut(j)] = column(g, j).astype(jnp.bfloat16)
            line_send(g, j).start()

    last = sp - 2

    def relay(i):
        for j in range(CHUNKS):
            if i <= last:
                stage_a(i, j)
            if i - 1 <= last:
                stage_b(i - 1, j)

    for j in range(CHUNKS):
        pcross[j].wait_recv()
        stream = stream_v[cut(j)] + pxr[cut(j)].astype(jnp.float32)
        stream_v[cut(j)] = stream
        nrm[z, t, cut(j), :width] = (
            stream
            * lax.rsqrt(jnp.mean(stream * stream, axis=-1, keepdims=True) + norm_eps)
            * gain_v[...]
        ).astype(jnp.bfloat16)
        stage_a(-1, j)

    @pl.when(short > 0)
    def _():
        for j in range(CHUNKS):
            for i in range(min(2, last + 1)):
                stage_a(i, j)
            stage_b(-1, j)
        for i in range(2, last + 1):
            for j in range(CHUNKS):
                stage_a(i, j)
        for j in range(CHUNKS):
            stage_b(0, j)

    @pl.when(short == 0)
    def _():
        relay(0)
        relay(1)

    stage_c(-1)
    stage_d(-1)
    for i in range(last + 1):
        if i + 2 <= last:

            @pl.when(short == 0)
            def _():
                for j in range(CHUNKS):
                    stage_a(i + 2, j)

        stage_c(i)
        stage_d(i)
        if i + 1 <= last:
            for j in range(CHUNKS):
                stage_b(i + 1, j)
        if i == last and i > 0:
            stage_f(0)
        stage_e(i)
    stage_e(-1)
    for i in range(0 if last == 0 else 1, last + 1):
        stage_f(i)
    @pl.when(z < sp - 1)
    def _():
        for copy in halo(True):
            copy.wait_send()

    @pl.when(z > 0)
    def _():
        for copy in halo(False):
            copy.wait_send()

    for copy in pcore + pcross:
        copy.wait_send()
    for i in range(-1, sp - 1):
        g = groups[i]
        part_send(g).wait_send()
        for j in range(CHUNKS):

            @pl.when((g <= z) & (z < sp - 1))
            def _():
                to_up(g, j).wait_send()

            @pl.when((g >= z) & (z > 0))
            def _():
                to_dn(g, j).wait_send()

            to_x(g, j).wait_send()
            to_core(g, t, j).wait_send()
            to_core(g, t_x, j).wait_send()
            if i >= 0:
                cross_send(g, j).wait_send()
            if 0 <= i < last:
                line_send(g, j).wait_send()

    for j in range(CHUNKS):
        stream_v[cut(j)] = stream_v[cut(j)] + column(z, j)
    for step in range(1, sp):
        src = groups[step - 1]
        for j in range(CHUNKS):
            rcopy(
                zsend.at[src, cut(j)],
                zrecv.at[src, cut(j)],
                zs_sem.at[src, j],
                zr_sem.at[src, j],
                at_z(src),
            ).wait_recv()
            total = stream_v[cut(j)] + zrecv[src, cut(j)].astype(jnp.float32)
            if step < sp - 1:
                stream_v[cut(j)] = total
            else:
                out_ref[cut(j)] = total.astype(out_ref.dtype)
    for j in range(CHUNKS):
        cross_send(z, j).wait_send()
        line_send(groups[last], j).wait_send()


def fused_scratch(sp, tp, shapes):
    (q, k, v, _, wo, res, gain, routes, gw, eg, eu, ed, sg, su, sd) = shapes
    rows, width = res.shape
    bf = jnp.bfloat16
    f32 = jnp.float32
    cross = tp // PAIR
    return [
        (q.shape, bf),
        (k.shape, bf),
        (v.shape, bf),
        (wo.shape, bf),
        (res.shape, bf),
        (gain.shape, f32),
        (routes.shape, jnp.int32),
        (gw.shape, f32),
        (eg.shape[1:], bf),
        (eu.shape[1:], bf),
        (ed.shape[1:], bf),
        (sg.shape, bf),
        (su.shape, bf),
        (sd.shape, bf),
        ((2,) + k.shape, bf),
        ((2,) + v.shape, bf),
        (q.shape, bf),
        ((tp, rows, width), f32),
        ((cross, rows, width), bf),
        ((cross, rows, width), bf),
        ((rows, width), bf),
        ((rows, width), bf),
        ((rows, width), f32),
        ((sp, tp, rows, width + LANES), bf),
        ((sp, PAIR, cross, rows, width), bf),
        ((sp, cross, rows, width), bf),
        ((sp, rows, width), bf),
        ((sp, rows, width), bf),
        ((sp, rows, width), bf),
        ((sp, rows, width), bf),
    ]


def size_of(shape, dtype):
    total = jnp.dtype(dtype).itemsize
    for extent in shape:
        total *= extent
    return total


def fused(sp, tp, buffers, *args):
    dma = pltpu.SemaphoreType.DMA
    any_spec = pl.BlockSpec(memory_space=pltpu.HBM)
    specs = [any_spec] * 15
    specs[3] = pl.BlockSpec(memory_space=pltpu.SMEM)
    res = args[5]
    return pl.pallas_call(
        functools.partial(fused_kernel, sp, tp),
        out_shape=pltpu.VMEM(res.shape, jnp.bfloat16),
        in_specs=specs,
        out_specs=pl.BlockSpec(memory_space=pltpu.VMEM),
        scratch_shapes=[pltpu.VMEM(s, d) for s, d in buffers]
        + [
            dma((14,)),
            dma((2, 2)),
            dma((2, 2)),
            dma((PAIR + CHUNKS,)),
            dma((PAIR + CHUNKS,)),
            dma((sp, tp, CHUNKS)),
            dma((sp, CHUNKS)),
            dma((sp, CHUNKS)),
            dma((sp, CHUNKS)),
            dma((sp, tp, CHUNKS)),
            dma((sp,)),
            dma((sp,)),
            dma((sp, CHUNKS)),
            dma((sp, CHUNKS)),
            dma((sp, CHUNKS)),
            dma((sp, CHUNKS)),
        ],
        compiler_params=pltpu.CompilerParams(
            collective_id=0, has_side_effects=True, vmem_limit_bytes=VMEM_BYTES
        ),
    )(*args)


def either(*args):
    sp = lax.axis_size("sp")
    tp = lax.axis_size("tp")
    args = list(args)
    shaped = list(args)
    shaped[6] = args[6].reshape(1, -1)
    shaped[7] = args[7].T
    shaped[8] = args[8].T
    buffers = fused_scratch(sp, tp, shaped)
    needed = sum(size_of(s, d) for s, d in buffers)
    fits = (
        2 * needed <= VMEM_BYTES
        and tp == 2 * PAIR
        and sp > 1
        and args[5].shape[0] % (16 * CHUNKS) == 0
        and 2 * sp * tp <= LANES
        and args[0].shape[0] == WINDOW
        and args[9].shape[0] == 1
    )
    if fits:
        return fused(sp, tp, buffers, *shaped)
    return body(*args)


def solution(mesh):
    placed = (
        P(("grp", "sp"), "tp"),
        P(("grp", "sp"), "tp"),
        P(("grp", "sp"), "tp"),
        P("tp"),
        P("tp", None),
        P(("grp", "sp", "tp"), None),
        P(),
        P(("grp", "sp", "tp"), None),
        P(("grp", "sp", "tp"), None),
        P(("sp", "tp"), None, None),
        P(("sp", "tp"), None, None),
        P(("sp", "tp"), None, None),
        P(None, "tp"),
        P(None, "tp"),
        P("tp", None),
    )
    return jax.shard_map(
        either, mesh=mesh, in_specs=placed, out_specs=P(("grp", "sp", "tp"), None), check_vma=False
    )
```

```python
import functools

import jax
import jax.numpy as jnp
from jax import lax
from jax.experimental import pallas as pl
from jax.experimental.pallas import tpu as pltpu
from jax.sharding import PartitionSpec as P

HEAD = 64
WINDOW = 128
TOPK = 6


norm_eps = 1e-06


def with_halo(block, sides, width):
    for axis, dim in sides:
        count = lax.axis_size(axis)
        forward = [(i, i + 1) for i in range(count - 1)]
        backward = [(target, source) for source, target in forward]
        low = lax.ppermute(
            lax.slice_in_dim(block, block.shape[dim] - width, None, axis=dim), axis, forward
        )
        high = lax.ppermute(lax.slice_in_dim(block, 0, width, axis=dim), axis, backward)
        block = jnp.concatenate([low, block, high], axis=dim)
    return block


def window_attention(query_rows, key_rows, value_rows, sink_logit):
    local_len = query_rows.shape[0]
    head_size = HEAD
    local_kv = key_rows.shape[1] // head_size
    local_heads = query_rows.shape[1] // head_size
    grouped = local_heads // local_kv
    blocks = local_len // WINDOW
    stacked = jnp.stack([key_rows, value_rows])
    widened = with_halo(stacked, (("sp", 1),), WINDOW)
    banded = widened.reshape(2, blocks + 2, WINDOW, local_kv, head_size)
    banded = jnp.concatenate([banded[:, :-2], banded[:, 1:-1], banded[:, 2:]], axis=2)
    queries = query_rows.reshape(blocks, WINDOW, local_kv, grouped, head_size)
    scores = jnp.einsum(
        "nqhgd,nkhd->nhgqk", queries, banded[0], preferred_element_type=jnp.float32
    ) * head_size ** (-0.5)
    seq_start = lax.axis_index("sp") * local_len
    total_len = lax.axis_size("sp") * local_len
    block_ids = jnp.arange(blocks, dtype=jnp.int32)[:, None, None]
    query_pos = seq_start + block_ids * WINDOW + jnp.arange(WINDOW, dtype=jnp.int32)[None, :, None]
    key_pos = (
        seq_start
        + (block_ids - 1) * WINDOW
        + jnp.arange(3 * WINDOW, dtype=jnp.int32)[None, None, :]
    )
    in_window = (jnp.abs(key_pos - query_pos) <= WINDOW) & (key_pos >= 0) & (key_pos < total_len)
    scores = jnp.where(in_window[:, None, None], scores, -jnp.inf)
    sink_part = sink_logit.reshape(1, local_kv, grouped, 1, 1)
    row_max = jnp.maximum(sink_part, jnp.max(scores, axis=-1, keepdims=True))
    shifted = jnp.exp(scores - row_max)
    denominator = jnp.exp(sink_part - row_max) + jnp.sum(shifted, axis=-1, keepdims=True)
    weights = (shifted / denominator).astype(jnp.bfloat16)
    attended = jnp.einsum(
        "nhgqk,nkhd->nqhgd", weights, banded[1], preferred_element_type=jnp.float32
    )
    return attended.astype(jnp.bfloat16).reshape(local_len, local_heads * head_size)


def body(
    query_rows,
    key_rows,
    value_rows,
    sink_logit,
    out_weight,
    residual,
    norm_gain,
    routes,
    gate_weights,
    expert_gate,
    expert_up,
    expert_down,
    shared_gate,
    shared_up,
    shared_down,
):
    attended = window_attention(query_rows, key_rows, value_rows, sink_logit)
    tok_dev = attended.shape[0]
    tok_rows = residual.shape[0]
    model_width = residual.shape[1]
    projected = lax.psum_scatter(
        jnp.dot(attended, out_weight, preferred_element_type=jnp.float32).astype(jnp.bfloat16),
        "tp",
        scatter_dimension=0,
        tiled=True,
    ).astype(jnp.float32)
    stream = residual.astype(jnp.float32) + projected
    normed = (
        stream * lax.rsqrt(jnp.mean(stream * stream, axis=-1, keepdims=True) + norm_eps) * norm_gain
    ).astype(jnp.bfloat16)
    sp_count = lax.axis_size("sp")
    tp_count = lax.axis_size("tp")
    experts_all = sp_count * tp_count
    capacity = (2 * tok_dev * TOPK + tp_count * experts_all - 1) // (tp_count * experts_all)
    copies = tok_rows * TOPK
    flat_expert = routes.reshape(-1)
    one_hot = (flat_expert[:, None] == jnp.arange(experts_all, dtype=jnp.int32)[None, :]).astype(
        jnp.int32
    )
    rank_in_expert = jnp.sum(jnp.cumsum(one_hot, axis=0) * one_hot, axis=1) - 1
    target_slot = flat_expert * capacity + rank_in_expert
    slot_token = (
        jnp.full((experts_all * capacity,), tok_rows, jnp.int32)
        .at[target_slot]
        .set(jnp.arange(copies, dtype=jnp.int32) // TOPK)
    )
    padded_rows = jnp.concatenate([normed, jnp.zeros((1, model_width), jnp.bfloat16)], axis=0)
    outgoing = padded_rows[slot_token].reshape(experts_all, capacity, model_width)
    incoming = lax.all_to_all(outgoing, ("sp", "tp"), split_axis=0, concat_axis=0, tiled=True)
    shaped = incoming.reshape(-1, model_width)
    gate_part = jnp.dot(shaped, expert_gate[0], preferred_element_type=jnp.float32)
    up_part = jnp.dot(shaped, expert_up[0], preferred_element_type=jnp.float32)
    hidden = (jax.nn.silu(gate_part) * up_part).astype(jnp.bfloat16)
    result = jnp.dot(hidden, expert_down[0], preferred_element_type=jnp.float32).astype(
        jnp.bfloat16
    )
    returned = lax.all_to_all(
        result.reshape(incoming.shape), ("sp", "tp"), split_axis=0, concat_axis=0, tiled=True
    )
    returned = returned.reshape(experts_all * capacity, model_width)
    gathered_copies = returned[target_slot].reshape(tok_rows, TOPK, model_width)
    routed = jnp.sum(gate_weights[:, :, None] * gathered_copies.astype(jnp.float32), axis=1)
    slab_rows = lax.all_gather(normed, "tp", axis=0, tiled=True)
    gate_part = jnp.dot(slab_rows, shared_gate, preferred_element_type=jnp.float32)
    up_part = jnp.dot(slab_rows, shared_up, preferred_element_type=jnp.float32)
    hidden = (jax.nn.silu(gate_part) * up_part).astype(jnp.bfloat16)
    partials = jnp.dot(hidden, shared_down, preferred_element_type=jnp.float32)
    shared = lax.psum_scatter(
        partials.astype(jnp.bfloat16), "tp", scatter_dimension=0, tiled=True
    ).astype(jnp.float32)
    return (stream + routed + shared).astype(jnp.bfloat16)


VMEM_BYTES = 66 * 1000 * 1000
PAIR = 2
LINE = 4
LANES = 128
CHUNKS = 2
SENDS = 20
DISPATCH_BY_LINE = ((0, 1),)
RETURN_BY_LINE = ((0, 2), (1, 0),)
RELAYS = {(0, 3): 2, (1, 3): 2}
ADDERS = {}
ORDER = {
    0: (
        ("N", 0),
        ("S", "o", 1, 0),
        ("N", 1),
        ("M", 0),
        ("S", "o", 2, 0),
        ("A", 1, "o", 0),
        ("M", 1),
        ("S", "o", 3, 0),
        ("S", "o", 2, 1),
        ("S", "m", 2, 0),
        ("S", "o", 3, 1),
        ("Q", 0),
        ("A", 1, "o", 1),
        ("S", "m", 1, 0),
        ("S", "m", 1, 1),
        ("S", "m", 2, 1),
        ("A", 2, "o", 0),
        ("Q", 2),
        ("A", 2, "o", 1),
        ("S", "o", 1, 1),
        ("A", 3, "o", 0),
        ("A", 3, "o", 1),
        ("A", 2, "m", 1),
        ("A", 1, "m", 0),
        ("A", 1, "m", 1),
        ("A", 2, "m", 0),
        ("S", "m", 3, 1),
        ("D", (1, 2)),
        ("E", 2),
        ("A", 3, "m", 1),
        ("A", 3, "m", 0),
        ("E", 1),
        ("D", (3,)),
        ("E", 3),
        ("S", "m", 3, 0),
        ("F", 3, 0),
        ("F", 3, 1),
        ("F", 1, 1),
        ("F", 1, 0),
        ("Q", 1),
        ("E", 0),
        ("F", 2, 1),
        ("G", 2, 1),
        ("H", 1),
        ("G", 3, 0),
        ("G", 1, 1),
        ("F", 2, 0),
        ("G", 1, 0),
        ("H", 0),
        ("G", 2, 0),
        ("G", 3, 1),
    ),
    1: (
        ("N", 0),
        ("S", "o", 2, 0),
        ("S", "o", 0, 0),
        ("N", 1),
        ("S", "o", 0, 1),
        ("S", "o", 3, 0),
        ("S", "o", 2, 1),
        ("M", 0),
        ("M", 1),
        ("A", 0, "o", 0),
        ("A", 2, "o", 0),
        ("S", "m", 2, 0),
        ("Q", 0),
        ("A", 2, "o", 1),
        ("A", 3, "o", 0),
        ("A", 3, "o", 1),
        ("A", 2, "m", 1),
        ("A", 0, "o", 1),
        ("A", 3, "m", 1),
        ("A", 0, "m", 0),
        ("A", 3, "m", 0),
        ("A", 2, "m", 0),
        ("A", 0, "m", 1),
        ("D", (0, 2, 3)),
        ("E", 2),
        ("E", 0),
        ("Q", 2),
        ("S", "m", 3, 1),
        ("Q", 1),
        ("S", "m", 0, 1),
        ("S", "o", 3, 1),
        ("F", 2, 0),
        ("E", 3),
        ("F", 0, 0),
        ("F", 3, 1),
        ("S", "m", 2, 1),
        ("F", 3, 0),
        ("S", "m", 0, 0),
        ("S", "m", 3, 0),
        ("E", 1),
        ("F", 2, 1),
        ("H", 0),
        ("H", 1),
        ("G", 0, 1),
        ("G", 3, 0),
        ("F", 0, 1),
        ("G", 2, 0),
        ("G", 2, 1),
        ("G", 3, 1),
        ("G", 0, 0),
    ),
}


def listed(source, target, pairs):
    mirrored = (LINE - 1 - source, LINE - 1 - target)
    return (source, target) in pairs or mirrored in pairs


def relay_of(source, target):
    if (source, target) in RELAYS:
        return RELAYS[(source, target)]
    mirrored = (LINE - 1 - source, LINE - 1 - target)
    if mirrored in RELAYS:
        return LINE - 1 - RELAYS[mirrored]
    return None


def adder_of(source, target):
    if listed(source, target, RETURN_BY_LINE):
        return None
    mirrored = (LINE - 1 - source, LINE - 1 - target)
    if (source, target) in ADDERS:
        adder = ADDERS[(source, target)]
    elif mirrored in ADDERS:
        adder = LINE - 1 - ADDERS[mirrored]
    else:
        return None
    return None if listed(adder, target, RETURN_BY_LINE) else adder


def silu(v):
    return v / (1.0 + jnp.exp(-v))


def fused_kernel(
    sp,
    tp,
    q_hbm,
    k_hbm,
    v_hbm,
    sink_hbm,
    wo_hbm,
    res_hbm,
    gain_hbm,
    routes_hbm,
    gw_hbm,
    eg_hbm,
    eu_hbm,
    ed_hbm,
    sg_hbm,
    su_hbm,
    sd_hbm,
    out_ref,
    q_v,
    k_v,
    v_v,
    sink_s,
    wo_v,
    res_v,
    gain_v,
    routes_v,
    gw_v,
    eg_v,
    eu_v,
    ed_v,
    sg_v,
    su_v,
    sd_v,
    eg_o,
    eu_o,
    ed_o,
    sg_o,
    su_o,
    sd_o,
    halo_k,
    halo_v,
    att_v,
    proj,
    psend,
    precv,
    pxs,
    pxr,
    pys,
    pyr,
    stream_v,
    mirror_v,
    tail_s,
    tail_m,
    nrm,
    part,
    xsend,
    xrecv,
    zsend,
    zrecv,
    zadd,
    load_sem,
    halo_r,
    pr_sem,
    w_s,
    w_r,
    send_sem,
    nrm_r,
    xr_sem,
    zr_sem,
    za_sem,
    far_sem,
):
    z = lax.axis_index("sp")
    t = lax.axis_index("tp")
    c = t % PAIR
    x = t // PAIR
    t_core = x * PAIR + (1 - c)
    t_x = (1 - x) * PAIR + c
    core = {"tp": t_core}
    xnbr = {"tp": t_x}
    upper = z // (sp // 2)

    def at_z(pos):
        return {"sp": pos}

    def rcopy(src, dst, ssem, rsem, dev):
        return pltpu.make_async_remote_copy(
            src_ref=src,
            dst_ref=dst,
            send_sem=ssem,
            recv_sem=rsem,
            device_id=dev,
            device_id_type=pl.DeviceIdType.MESH,
        )

    def signal(sem, dev):
        pl.semaphore_signal(sem, inc=1, device_id=dev, device_id_type=pl.DeviceIdType.MESH)

    moves = [
        (k_hbm, k_v),
        (v_hbm, v_v),
        (q_hbm, q_v),
        (sink_hbm, sink_s),
        (routes_hbm, routes_v),
        (gw_hbm, gw_v),
        (wo_hbm, wo_v),
        (res_hbm, res_v),
        (gain_hbm, gain_v),
        (sg_hbm, sg_v),
        (su_hbm, su_v),
        (sd_hbm, sd_v),
        (eg_hbm.at[0], eg_v),
        (eu_hbm.at[0], eu_v),
        (ed_hbm.at[0], ed_v),
    ]
    early = 9
    loads = [
        pltpu.make_async_copy(a, b, load_sem.at[i if i < early else i - early])
        for i, (a, b) in enumerate(moves)
    ]
    pending = []

    def sent(copy, condition=None):
        pending.append((copy, condition))

    def slot():
        if len(pending) >= SENDS:
            settle(pending[len(pending) - SENDS])
        return send_sem.at[len(pending) % SENDS]

    def settle(entry):
        copy, condition = entry
        if condition is None:
            copy.wait_send()
        else:
            pl.when(condition)(copy.wait_send)

    barrier = pltpu.get_barrier_semaphore()
    for dev in (core, xnbr):
        signal(barrier, dev)

    @pl.when(z > 0)
    def _():
        signal(barrier, at_z(z - 1))

    @pl.when(z < sp - 1)
    def _():
        signal(barrier, at_z(z + 1))

    for load in loads[:early]:
        load.start()
    rows = stream_v.shape[0]
    width = stream_v.shape[1]
    length = q_v.shape[0]
    heads = q_v.shape[1] // HEAD
    kv_heads = k_v.shape[1] // HEAD
    grouped = heads // kv_heads

    @pl.when(z == 0)
    def _():
        halo_k[0] = jnp.zeros(halo_k.shape[1:], halo_k.dtype)
        halo_v[0] = jnp.zeros(halo_v.shape[1:], halo_v.dtype)

    @pl.when(z == sp - 1)
    def _():
        halo_k[1] = jnp.zeros(halo_k.shape[1:], halo_k.dtype)
        halo_v[1] = jnp.zeros(halo_v.shape[1:], halo_v.dtype)

    loads[0].wait()
    loads[1].wait()
    peers = 2 + jnp.where(z > 0, 1, 0) + jnp.where(z < sp - 1, 1, 0)
    pl.semaphore_wait(barrier, peers)

    def halo(up, which, sem):
        pos = z + 1 if up else z - 1
        row = 0 if up else 1
        src = (k_v, v_v)[which]
        dst = (halo_k, halo_v)[which]
        return rcopy(src, dst.at[row], sem, halo_r.at[row, which], at_z(pos))

    def halo_wait(row, which):
        src = (k_v, v_v)[which]
        dst = (halo_k, halo_v)[which]
        rcopy(src, dst.at[row], send_sem.at[0], halo_r.at[row, which], core).wait_recv()

    for which in range(2):
        for up, condition in ((True, z < sp - 1), (False, z > 0)):
            copy = halo(up, which, slot())
            pl.when(condition)(copy.start)
            sent(copy, condition)

    def push(i, src, dst):
        return rcopy(src, dst, w_s.at[i], w_r.at[i], core)

    pushes = [
        push(0, eg_hbm.at[0], eg_o),
        push(1, sg_hbm, sg_o),
        push(2, su_hbm, su_o),
        push(3, sd_hbm, sd_o),
        push(4, eu_hbm.at[0], eu_o),
        push(5, ed_hbm.at[0], ed_o),
    ]
    for copy in pushes[:2]:
        copy.start()

    for k in range(2, 6):
        loads[k].wait()
    for load in loads[early:]:
        load.start()
    half = LANES // 2
    lane = lax.broadcasted_iota(jnp.int32, (rows, LANES), 1)
    unit = lax.broadcasted_iota(jnp.int32, (LANES, rows), 0)
    unit = jnp.where(unit < half, unit, unit - half)
    combine = jnp.zeros((LANES, rows), jnp.float32)
    for k in range(TOPK):
        combine = combine + jnp.where(routes_v[k : k + 1] == unit, gw_v[k : k + 1], 0.0)
    combine = combine.T
    high = combine.astype(jnp.bfloat16)
    low = (combine - high.astype(jnp.float32)).astype(jnp.bfloat16)
    own_tail = jnp.where(
        lane < half, high.astype(jnp.float32), low.astype(jnp.float32)
    ).astype(jnp.bfloat16)
    nrm[z, x, :, width:] = own_tail
    tail_s[...] = own_tail
    tail_copy = rcopy(tail_s, tail_m, slot(), w_r.at[6], xnbr)
    tail_copy.start()
    sent(tail_copy)

    contract = (((1,), (1,)), ((), ()))
    scale = HEAD ** (-0.5)

    def cols(head):
        return slice(head * HEAD, (head + 1) * HEAD)

    def stacked(kv):
        first = kv * grouped
        return jnp.concatenate(
            [q_v[:, cols(first + i)] for i in range(grouped)], axis=0
        ) * jnp.asarray(scale, q_v.dtype)

    def product(a, b):
        return lax.dot_general(a, b, contract, preferred_element_type=jnp.float32)

    queries = [stacked(kv) for kv in range(kv_heads)]
    row = lax.broadcasted_iota(jnp.int32, (grouped * length, 1), 0)
    tops = []
    sums = []
    outs = []
    for kv in range(kv_heads):
        scores = product(queries[kv], k_v[:, cols(kv)])
        sink = jnp.full((grouped * length, 1), sink_s[kv * grouped], jnp.float32)
        for i in range(1, grouped):
            sink = jnp.where(row >= i * length, sink_s[kv * grouped + i], sink)
        top = jnp.maximum(jnp.max(scores, axis=-1, keepdims=True), sink)
        e = jnp.exp(scores - top)
        tops.append(top)
        sums.append(jnp.exp(sink - top) + jnp.sum(e, axis=-1, keepdims=True))
        outs.append(
            jnp.dot(e.astype(jnp.bfloat16), v_v[:, cols(kv)], preferred_element_type=jnp.float32)
        )

    qi = lax.broadcasted_iota(jnp.int32, (grouped * length, length), 0) % length
    ki = lax.broadcasted_iota(jnp.int32, (grouped * length, length), 1)
    low_bound = jnp.where(z > 0, 0, length)
    high_bound = jnp.where(z < sp - 1, 0, length)
    low_mask = ki - qi >= low_bound
    high_mask = qi - ki >= high_bound

    def wait_halo(which):
        @pl.when(z > 0)
        def _():
            halo_wait(0, which)

        @pl.when(z < sp - 1)
        def _():
            halo_wait(1, which)

    wait_halo(0)
    sides = []
    for kv in range(kv_heads):
        s_low = jnp.where(low_mask, product(queries[kv], halo_k[0, :, cols(kv)]), -jnp.inf)
        s_high = jnp.where(high_mask, product(queries[kv], halo_k[1, :, cols(kv)]), -jnp.inf)
        top = jnp.max(jnp.maximum(s_low, s_high), axis=-1, keepdims=True)
        top = jnp.maximum(top, tops[kv])
        e_low = jnp.exp(s_low - top)
        e_high = jnp.exp(s_high - top)
        shrink = jnp.exp(tops[kv] - top)
        denominator = shrink * sums[kv] + jnp.sum(e_low + e_high, axis=-1, keepdims=True)
        sides.append(
            (
                shrink * outs[kv],
                e_low.astype(jnp.bfloat16),
                e_high.astype(jnp.bfloat16),
                1.0 / denominator,
            )
        )
    wait_halo(1)
    for kv in range(kv_heads):
        base, e_low, e_high, inverse = sides[kv]
        base = base + jnp.dot(
            e_low, halo_v[0, :, cols(kv)], preferred_element_type=jnp.float32
        )
        base = base + jnp.dot(
            e_high, halo_v[1, :, cols(kv)], preferred_element_type=jnp.float32
        )
        base = (base * inverse).astype(jnp.bfloat16)
        for i in range(grouped):
            att_v[:, :, cols(kv * grouped + i)] = base[i * length : (i + 1) * length].reshape(
                tp, rows, HEAD
            )

    @pl.when(z == 1)
    def _():
        signal(far_sem, at_z(z - 1))

    @pl.when(z == sp - 2)
    def _():
        signal(far_sem, at_z(z + 1))

    loads[6].wait()

    def projected(cc):
        picked = jnp.concatenate([att_v[xh * PAIR + cc] for xh in range(PAIR)], axis=0)
        return jnp.dot(picked, wo_v[...], preferred_element_type=jnp.float32)

    psend[...] = projected(1 - c).astype(jnp.bfloat16).reshape(psend.shape)
    pcore = []
    for order, xx in enumerate((1 - x, x)):
        pcore.append(rcopy(psend.at[xx], precv.at[xx], slot(), pr_sem.at[order], core))
        pcore[-1].start()
        sent(pcore[-1])
    for copy in pushes[2:]:
        copy.start()
    proj[...] = projected(c).reshape(proj.shape)
    piece = rows // CHUNKS

    def cut(j):
        return pl.ds(j * piece, piece)

    def cross(src, dst, k):
        copy = rcopy(src, dst, slot(), pr_sem.at[PAIR + k], xnbr)
        copy.start()
        sent(copy)
        return copy

    pcore[0].wait_recv()
    mirror_v[...] = proj[1 - x] + precv[1 - x].astype(jnp.float32)
    pcross = []
    for j in range(CHUNKS):
        pxs[cut(j)] = mirror_v[cut(j)].astype(jnp.bfloat16)
        pcross.append(cross(pxs.at[cut(j)], pxr.at[cut(j)], j))
    loads[7].wait()
    loads[8].wait()
    pcore[1].wait_recv()
    stream_v[...] = res_v[...].astype(jnp.float32) + proj[x] + precv[x].astype(jnp.float32)
    pmirror = []
    for j in range(CHUNKS):
        pys[cut(j)] = stream_v[cut(j)].astype(jnp.bfloat16)
        pmirror.append(cross(pys.at[cut(j)], pyr.at[cut(j)], CHUNKS + j))
    tail_copy.wait_recv()
    nrm[z, 1 - x, :, width:] = tail_m[...]

    def normalized(stream):
        return (
            stream
            * lax.rsqrt(jnp.mean(stream * stream, axis=-1, keepdims=True) + norm_eps)
            * gain_v[...]
        ).astype(jnp.bfloat16)

    expert = z * tp + t
    sibling = z * tp + t_core

    def schedule(me):
        def place(p):
            return p + upper * (sp - 1 - 2 * p)

        def send(src, dst, rsem, dev):
            copy = rcopy(src, dst, slot(), rsem, dev)
            copy.start()
            sent(copy)

        def side(h):
            return x if h == "o" else 1 - x

        def block_send(p, h, j, dev):
            g = place(p)
            ref = nrm.at[g, side(h), cut(j)]
            send(ref, ref, nrm_r.at[g, side(h), j], dev)

        def block_wait(p, h, j):
            g = place(p)
            ref = nrm.at[g, side(h), cut(j)]
            rcopy(ref, ref, send_sem.at[0], nrm_r.at[g, side(h), j], core).wait_recv()

        def cross_copy(p, j, sem):
            g = place(p)
            return rcopy(
                xsend.at[g, cut(j)], xrecv.at[g, cut(j)], sem, xr_sem.at[g, j], xnbr
            )

        lane_of = {"o": 0, "m": 1}

        def line_send(p, h, span):
            g = place(p)
            send(
                zsend.at[g, side(h), span],
                zrecv.at[z, side(h), span],
                zr_sem.at[z, lane_of[h]],
                at_z(g),
            )

        def line_wait(p, h):
            g = place(p)
            ref = zrecv.at[g, side(h)]
            rcopy(ref, ref, send_sem.at[0], zr_sem.at[g, lane_of[h]], core).wait_recv()
            return zrecv[g, side(h)].astype(jnp.float32)

        def add_send(p, j, adder):
            g = place(p)
            send(
                zsend.at[g, x, cut(j)], zadd.at[g, cut(j)], za_sem.at[g, j], at_z(place(adder))
            )

        def add_wait(p, j):
            g = place(p)
            ref = zadd.at[g, cut(j)]
            rcopy(ref, ref, send_sem.at[0], za_sem.at[g, j], core).wait_recv()
            return zadd[g, cut(j)].astype(jnp.float32)

        def cross_wait(p, j):
            cross_copy(p, j, send_sem.at[0]).wait_recv()
            g = place(p)
            return part[g, x, cut(j)] + xrecv[g, cut(j)].astype(jnp.float32)

        waited = set()

        def once(name, copies):
            if name not in waited:
                waited.add(name)
                for copy in copies:
                    copy()

        def own_weights():
            once("own", [loads[k].wait for k in range(9, 15)])

        def sibling_experts():
            once("experts", [pushes[k].wait_recv for k in (0, 4, 5)])

        def sibling_shared():
            once("shared", [pushes[k].wait_recv for k in (1, 2, 3)])

        def one(acts, gate_ref, up_ref, down_ref):
            gate = jnp.dot(acts, gate_ref[...], preferred_element_type=jnp.float32)
            up = jnp.dot(acts, up_ref[...], preferred_element_type=jnp.float32)
            hidden = (silu(gate) * up).astype(jnp.bfloat16)
            out = jnp.dot(hidden, down_ref[...], preferred_element_type=jnp.float32)
            return out.astype(jnp.bfloat16).astype(jnp.float32)

        def rows_of(places):
            block = [nrm[g].reshape(PAIR * rows, nrm.shape[-1]) for g in places]
            block = jnp.concatenate(block * 2 if len(block) == 1 else block, axis=0)
            return block[:, :width], block[:, width:].astype(jnp.float32)

        def weight(tail, e):
            lanes = lax.broadcasted_iota(jnp.int32, tail.shape, 1)
            mine = (lanes == e) | (lanes == e + half)
            return jnp.sum(jnp.where(mine, tail, 0.0), axis=-1, keepdims=True)

        def experts(ps):
            own_weights()
            sibling_experts()
            places = [place(p) for p in ps]
            acts, tail = rows_of(places)
            result = weight(tail, expert) * one(acts, eg_v, eu_v, ed_v)
            result = result + weight(tail, sibling) * one(acts, eg_o, eu_o, ed_o)
            result = result[: len(ps) * PAIR * rows].reshape(len(ps), PAIR, rows, width)
            for i, g in enumerate(places):
                part[g] = result[i]

        own_parts = [op for op in ORDER[me] if op[0] == "Q"]

        def own_part(op):
            own_weights()
            acts, tail = rows_of([z])
            if op[1] == 0:
                result = weight(tail, expert) * one(acts, eg_v, eu_v, ed_v)
            elif op[1] == 1:
                sibling_experts()
                result = weight(tail, sibling) * one(acts, eg_o, eu_o, ed_o)
            else:
                sibling_shared()
                result = one(acts, sg_v, su_v, sd_v) + one(acts, sg_o, su_o, sd_o)
            result = result[: PAIR * rows].reshape(PAIR, rows, width)
            if op == own_parts[0]:
                part[z] = result
            else:
                part[z] = part[z] + result

        knows_far = False
        summed = set()
        tail_from = None
        for op in ORDER[me]:
            kind = op[0]
            if kind == "E" and tail_from is None:
                tail_from = len(pending)
            if kind in "HG" and not summed:
                for entry in pending[max(0, len(pending) - SENDS) : tail_from]:
                    settle(entry)
                for copy in pushes:
                    copy.wait_send()
                settled = max(tail_from, len(pending) - SENDS)
                summed.add(me)
            with jax.named_scope("op_" + "_".join(str(v) for v in op)):
                if kind == "N":
                    j = op[1]
                    pcross[j].wait_recv()
                    stream = stream_v[cut(j)] + pxr[cut(j)].astype(jnp.float32)
                    stream_v[cut(j)] = stream
                    nrm[z, x, cut(j), :width] = normalized(stream)
                elif kind == "M":
                    j = op[1]
                    pmirror[j].wait_recv()
                    stream = mirror_v[cut(j)] + pyr[cut(j)].astype(jnp.float32)
                    nrm[z, 1 - x, cut(j), :width] = normalized(stream)
                elif kind == "S":
                    h, p, j = op[1:]
                    if relay_of(me, p) is None and (
                        h == "o" or listed(me, p, DISPATCH_BY_LINE)
                    ):
                        if me == 0 and p == LINE - 1 and not knows_far:
                            pl.semaphore_wait(far_sem, 1)
                            knows_far = True
                        block_send(me, h, j, at_z(place(p)))
                elif kind == "A":
                    p, h, j = op[1:]
                    block_wait(p, h, j)
                    mirrored_in = listed(p, me, DISPATCH_BY_LINE)
                    if h == "o" and not mirrored_in:
                        block_send(p, h, j, xnbr)
                    for q in range(LINE):
                        if q not in (p, me) and relay_of(p, q) == me:
                            if h == "o" or (mirrored_in and listed(p, q, DISPATCH_BY_LINE)):
                                block_send(p, h, j, at_z(place(q)))
                elif kind == "D":
                    experts(op[1])
                elif kind == "Q":
                    own_part(op)
                elif kind == "E":
                    p = op[1]
                    g = place(p)
                    if p != me and listed(me, p, RETURN_BY_LINE):
                        for h in ("o", "m"):
                            zsend[g, side(h)] = part[g, side(h)].astype(jnp.bfloat16)
                            line_send(p, h, slice(None))
                    else:
                        if p == me:
                            for q in range(LINE):
                                if q != me and listed(q, me, RETURN_BY_LINE):
                                    part[g, 1 - x] = part[g, 1 - x] + line_wait(q, "m")
                        for j in range(CHUNKS):
                            xsend[g, cut(j)] = part[g, 1 - x, cut(j)].astype(jnp.bfloat16)
                            copy = cross_copy(p, j, slot())
                            copy.start()
                            sent(copy)
                elif kind == "F":
                    p, j = op[1:]
                    if not listed(me, p, RETURN_BY_LINE):
                        value = cross_wait(p, j)
                        for q in range(LINE):
                            if q not in (p, me) and adder_of(q, p) == me:
                                value = value + add_wait(p, j)
                        zsend[place(p), x, cut(j)] = value.astype(jnp.bfloat16)
                        adder = adder_of(me, p)
                        if adder is None:
                            line_send(p, "o", cut(j))
                        else:
                            add_send(p, j, adder)
                elif kind == "H":
                    j = op[1]
                    stream_v[cut(j)] = stream_v[cut(j)] + cross_wait(me, j)
                elif kind == "G":
                    p = op[1]
                    if p not in summed and adder_of(p, me) is None:
                        stream_v[...] = stream_v[...] + line_wait(p, "o")
                    summed.add(p)
        out_ref[...] = stream_v[...].astype(out_ref.dtype)
        if me == 0 and not knows_far:
            pl.semaphore_wait(far_sem, 1)
        with jax.named_scope("lastwaits"):
            for entry in pending[settled:]:
                settle(entry)

    shared_pending = list(pending)
    for me in range(LINE // 2):

        @pl.when((z == me) | (z == sp - 1 - me))
        def _():
            pending[:] = shared_pending
            schedule(me)


def fused_scratch(sp, tp, shapes):
    (q, k, v, sink, wo, res, gain, routes, gw, eg, eu, ed, sg, su, sd) = shapes
    rows, width = res.shape
    bf = jnp.bfloat16
    f32 = jnp.float32
    return [
        (q.shape, bf),
        (k.shape, bf),
        (v.shape, bf),
        (sink.shape, f32),
        (wo.shape, bf),
        (res.shape, bf),
        (gain.shape, f32),
        (routes.shape, jnp.int32),
        (gw.shape, f32),
        (eg.shape[1:], bf),
        (eu.shape[1:], bf),
        (ed.shape[1:], bf),
        (sg.shape, bf),
        (su.shape, bf),
        (sd.shape, bf),
        (eg.shape[1:], bf),
        (eu.shape[1:], bf),
        (ed.shape[1:], bf),
        (sg.shape, bf),
        (su.shape, bf),
        (sd.shape, bf),
        ((2,) + k.shape, bf),
        ((2,) + v.shape, bf),
        ((tp, rows, q.shape[1]), bf),
        ((PAIR, rows, width), f32),
        ((PAIR, rows, width), bf),
        ((PAIR, rows, width), bf),
        ((rows, width), bf),
        ((rows, width), bf),
        ((rows, width), bf),
        ((rows, width), bf),
        ((rows, width), f32),
        ((rows, width), f32),
        ((rows, LANES), bf),
        ((rows, LANES), bf),
        ((sp, PAIR, rows, width + LANES), bf),
        ((sp, PAIR, rows, width), f32),
        ((sp, rows, width), bf),
        ((sp, rows, width), bf),
        ((sp, PAIR, rows, width), bf),
        ((sp, PAIR, rows, width), bf),
        ((sp, rows, width), bf),
    ]


def size_of(shape, dtype):
    total = jnp.dtype(dtype).itemsize
    for extent in shape:
        total *= extent
    return total


def fused(sp, tp, buffers, *args):
    dma = pltpu.SemaphoreType.DMA
    res = args[5]
    scratch = [pltpu.VMEM(s, d) for s, d in buffers]
    scratch[3] = pltpu.SMEM(*buffers[3])
    return pl.pallas_call(
        functools.partial(fused_kernel, sp, tp),
        out_shape=pltpu.VMEM(res.shape, jnp.bfloat16),
        in_specs=[pl.BlockSpec(memory_space=pltpu.HBM)] * 15,
        out_specs=pl.BlockSpec(memory_space=pltpu.VMEM),
        scratch_shapes=scratch
        + [
            dma((9,)),
            dma((2, 2)),
            dma((PAIR + 2 * CHUNKS,)),
            dma((6,)),
            dma((7,)),
            dma((SENDS,)),
            dma((sp, PAIR, CHUNKS)),
            dma((sp, CHUNKS)),
            dma((sp, PAIR)),
            dma((sp, CHUNKS)),
            pltpu.SemaphoreType.REGULAR,
        ],
        compiler_params=pltpu.CompilerParams(
            collective_id=0, has_side_effects=True, vmem_limit_bytes=VMEM_BYTES
        ),
    )(*args)


def either(*args):
    sp = lax.axis_size("sp")
    tp = lax.axis_size("tp")
    args = list(args)
    shaped = list(args)
    shaped[6] = args[6].reshape(1, -1)
    shaped[7] = args[7].T
    shaped[8] = args[8].T
    buffers = fused_scratch(sp, tp, shaped)
    needed = sum(size_of(s, d) for s, d in buffers)
    fits = (
        2 * needed <= VMEM_BYTES
        and tp == 2 * PAIR
        and sp == LINE
        and args[5].shape[0] % (16 * CHUNKS) == 0
        and 2 * sp * tp <= LANES
        and args[0].shape[0] == WINDOW
        and args[9].shape[0] == 1
    )
    if fits:
        return fused(sp, tp, buffers, *shaped)
    return body(*args)


def solution(mesh):
    placed = (
        P(("grp", "sp"), "tp"),
        P(("grp", "sp"), "tp"),
        P(("grp", "sp"), "tp"),
        P("tp"),
        P("tp", None),
        P(("grp", "sp", "tp"), None),
        P(),
        P(("grp", "sp", "tp"), None),
        P(("grp", "sp", "tp"), None),
        P(("sp", "tp"), None, None),
        P(("sp", "tp"), None, None),
        P(("sp", "tp"), None, None),
        P(None, "tp"),
        P(None, "tp"),
        P("tp", None),
    )
    return jax.shard_map(
        either, mesh=mesh, in_specs=placed, out_specs=P(("grp", "sp", "tp"), None), check_vma=False
    )
```

```python
import functools

import jax
import jax.numpy as jnp
from jax import lax
from jax.experimental import pallas as pl
from jax.experimental.pallas import tpu as pltpu
from jax.sharding import PartitionSpec as P

HEAD = 64
WINDOW = 128
TOPK = 6


norm_eps = 1e-06


def with_halo(block, sides, width):
    for axis, dim in sides:
        count = lax.axis_size(axis)
        forward = [(i, i + 1) for i in range(count - 1)]
        backward = [(target, source) for source, target in forward]
        low = lax.ppermute(
            lax.slice_in_dim(block, block.shape[dim] - width, None, axis=dim), axis, forward
        )
        high = lax.ppermute(lax.slice_in_dim(block, 0, width, axis=dim), axis, backward)
        block = jnp.concatenate([low, block, high], axis=dim)
    return block


def window_attention(query_rows, key_rows, value_rows, sink_logit):
    local_len = query_rows.shape[0]
    head_size = HEAD
    local_kv = key_rows.shape[1] // head_size
    local_heads = query_rows.shape[1] // head_size
    grouped = local_heads // local_kv
    blocks = local_len // WINDOW
    stacked = jnp.stack([key_rows, value_rows])
    widened = with_halo(stacked, (("sp", 1),), WINDOW)
    banded = widened.reshape(2, blocks + 2, WINDOW, local_kv, head_size)
    banded = jnp.concatenate([banded[:, :-2], banded[:, 1:-1], banded[:, 2:]], axis=2)
    queries = query_rows.reshape(blocks, WINDOW, local_kv, grouped, head_size)
    scores = jnp.einsum(
        "nqhgd,nkhd->nhgqk", queries, banded[0], preferred_element_type=jnp.float32
    ) * head_size ** (-0.5)
    seq_start = lax.axis_index("sp") * local_len
    total_len = lax.axis_size("sp") * local_len
    block_ids = jnp.arange(blocks, dtype=jnp.int32)[:, None, None]
    query_pos = seq_start + block_ids * WINDOW + jnp.arange(WINDOW, dtype=jnp.int32)[None, :, None]
    key_pos = (
        seq_start
        + (block_ids - 1) * WINDOW
        + jnp.arange(3 * WINDOW, dtype=jnp.int32)[None, None, :]
    )
    in_window = (jnp.abs(key_pos - query_pos) <= WINDOW) & (key_pos >= 0) & (key_pos < total_len)
    scores = jnp.where(in_window[:, None, None], scores, -jnp.inf)
    sink_part = sink_logit.reshape(1, local_kv, grouped, 1, 1)
    row_max = jnp.maximum(sink_part, jnp.max(scores, axis=-1, keepdims=True))
    shifted = jnp.exp(scores - row_max)
    denominator = jnp.exp(sink_part - row_max) + jnp.sum(shifted, axis=-1, keepdims=True)
    weights = (shifted / denominator).astype(jnp.bfloat16)
    attended = jnp.einsum(
        "nhgqk,nkhd->nqhgd", weights, banded[1], preferred_element_type=jnp.float32
    )
    return attended.astype(jnp.bfloat16).reshape(local_len, local_heads * head_size)


def body(
    query_rows,
    key_rows,
    value_rows,
    sink_logit,
    out_weight,
    residual,
    norm_gain,
    routes,
    gate_weights,
    expert_gate,
    expert_up,
    expert_down,
    shared_gate,
    shared_up,
    shared_down,
):
    attended = window_attention(query_rows, key_rows, value_rows, sink_logit)
    tok_dev = attended.shape[0]
    tok_rows = residual.shape[0]
    model_width = residual.shape[1]
    projected = lax.psum_scatter(
        jnp.dot(attended, out_weight, preferred_element_type=jnp.float32).astype(jnp.bfloat16),
        "tp",
        scatter_dimension=0,
        tiled=True,
    ).astype(jnp.float32)
    stream = residual.astype(jnp.float32) + projected
    normed = (
        stream * lax.rsqrt(jnp.mean(stream * stream, axis=-1, keepdims=True) + norm_eps) * norm_gain
    ).astype(jnp.bfloat16)
    sp_count = lax.axis_size("sp")
    tp_count = lax.axis_size("tp")
    experts_all = sp_count * tp_count
    capacity = (2 * tok_dev * TOPK + tp_count * experts_all - 1) // (tp_count * experts_all)
    copies = tok_rows * TOPK
    flat_expert = routes.reshape(-1)
    one_hot = (flat_expert[:, None] == jnp.arange(experts_all, dtype=jnp.int32)[None, :]).astype(
        jnp.int32
    )
    rank_in_expert = jnp.sum(jnp.cumsum(one_hot, axis=0) * one_hot, axis=1) - 1
    target_slot = flat_expert * capacity + rank_in_expert
    slot_token = (
        jnp.full((experts_all * capacity,), tok_rows, jnp.int32)
        .at[target_slot]
        .set(jnp.arange(copies, dtype=jnp.int32) // TOPK)
    )
    padded_rows = jnp.concatenate([normed, jnp.zeros((1, model_width), jnp.bfloat16)], axis=0)
    outgoing = padded_rows[slot_token].reshape(experts_all, capacity, model_width)
    incoming = lax.all_to_all(outgoing, ("sp", "tp"), split_axis=0, concat_axis=0, tiled=True)
    shaped = incoming.reshape(-1, model_width)
    gate_part = jnp.dot(shaped, expert_gate[0], preferred_element_type=jnp.float32)
    up_part = jnp.dot(shaped, expert_up[0], preferred_element_type=jnp.float32)
    hidden = (jax.nn.silu(gate_part) * up_part).astype(jnp.bfloat16)
    result = jnp.dot(hidden, expert_down[0], preferred_element_type=jnp.float32).astype(
        jnp.bfloat16
    )
    returned = lax.all_to_all(
        result.reshape(incoming.shape), ("sp", "tp"), split_axis=0, concat_axis=0, tiled=True
    )
    returned = returned.reshape(experts_all * capacity, model_width)
    gathered_copies = returned[target_slot].reshape(tok_rows, TOPK, model_width)
    routed = jnp.sum(gate_weights[:, :, None] * gathered_copies.astype(jnp.float32), axis=1)
    slab_rows = lax.all_gather(normed, "tp", axis=0, tiled=True)
    gate_part = jnp.dot(slab_rows, shared_gate, preferred_element_type=jnp.float32)
    up_part = jnp.dot(slab_rows, shared_up, preferred_element_type=jnp.float32)
    hidden = (jax.nn.silu(gate_part) * up_part).astype(jnp.bfloat16)
    partials = jnp.dot(hidden, shared_down, preferred_element_type=jnp.float32)
    shared = lax.psum_scatter(
        partials.astype(jnp.bfloat16), "tp", scatter_dimension=0, tiled=True
    ).astype(jnp.float32)
    return (stream + routed + shared).astype(jnp.bfloat16)


VMEM_BYTES = 66 * 1000 * 1000
PAIR = 2
LINE = 4
LANES = 128
CHUNKS = 2
SENDS = 20
DISPATCH_BY_LINE = ()
RETURN_BY_LINE = ((0, 1), (1, 3),)
RELAYS = {(0, 2): 1, (0, 3): 2, (1, 3): 2}
ADDERS = {(0, 2): 1, (0, 3): 1}
ORDER = {
    0: (
        ("N", 1),
        ("N", 0),
        ("S", "o", 1, 1),
        ("A", 1, "o", 0),
        ("S", "o", 1, 0),
        ("A", 1, "o", 1),
        ("A", 1, "m", 0),
        ("A", 1, "m", 1),
        ("A", 2, "o", 0),
        ("A", 2, "o", 1),
        ("D", (1,)),
        ("M", 0),
        ("M", 1),
        ("E", 1),
        ("A", 2, "m", 0),
        ("A", 3, "o", 0),
        ("F", 1, 0),
        ("A", 3, "o", 1),
        ("A", 2, "m", 1),
        ("D", (2,)),
        ("E", 2),
        ("S", "o", 2, 1),
        ("A", 3, "m", 0),
        ("S", "m", 1, 0),
        ("A", 3, "m", 1),
        ("S", "m", 2, 1),
        ("S", "o", 3, 1),
        ("D", (3,)),
        ("F", 2, 0),
        ("E", 3),
        ("Q", 1),
        ("F", 2, 1),
        ("Q", 0),
        ("F", 3, 0),
        ("S", "m", 3, 1),
        ("Q", 2),
        ("F", 1, 1),
        ("S", "m", 2, 0),
        ("G", 2, 1),
        ("F", 3, 1),
        ("E", 0),
        ("G", 1, 0),
        ("S", "m", 1, 1),
        ("H", 0),
        ("S", "m", 3, 0),
        ("G", 2, 0),
        ("G", 3, 0),
        ("S", "o", 3, 0),
        ("G", 3, 1),
        ("H", 1),
        ("G", 1, 1),
        ("S", "o", 2, 0),
    ),
    1: (
        ("N", 0),
        ("S", "o", 0, 0),
        ("S", "o", 2, 0),
        ("N", 1),
        ("M", 0),
        ("S", "o", 0, 1),
        ("S", "o", 2, 1),
        ("A", 2, "o", 0),
        ("S", "o", 3, 1),
        ("M", 1),
        ("A", 0, "o", 1),
        ("S", "m", 3, 1),
        ("S", "m", 2, 1),
        ("A", 2, "o", 1),
        ("A", 0, "o", 0),
        ("Q", 2),
        ("A", 3, "o", 0),
        ("A", 3, "o", 1),
        ("A", 3, "m", 1),
        ("A", 2, "m", 0),
        ("A", 3, "m", 0),
        ("D", (3,)),
        ("S", "m", 0, 1),
        ("A", 0, "m", 1),
        ("E", 3),
        ("A", 0, "m", 0),
        ("A", 2, "m", 1),
        ("S", "m", 2, 0),
        ("S", "o", 3, 0),
        ("D", (0, 2)),
        ("E", 0),
        ("Q", 1),
        ("G", 3, 1),
        ("E", 2),
        ("Q", 0),
        ("F", 2, 0),
        ("F", 0, 0),
        ("E", 1),
        ("F", 3, 1),
        ("F", 0, 1),
        ("F", 2, 1),
        ("G", 0, 0),
        ("H", 1),
        ("H", 0),
        ("G", 2, 0),
        ("S", "m", 0, 0),
        ("G", 0, 1),
        ("G", 3, 0),
        ("F", 3, 0),
        ("G", 2, 1),
        ("S", "m", 3, 0),
    ),
}


def listed(source, target, pairs):
    mirrored = (LINE - 1 - source, LINE - 1 - target)
    return (source, target) in pairs or mirrored in pairs


def relay_of(source, target):
    if (source, target) in RELAYS:
        return RELAYS[(source, target)]
    mirrored = (LINE - 1 - source, LINE - 1 - target)
    if mirrored in RELAYS:
        return LINE - 1 - RELAYS[mirrored]
    return None


def adder_of(source, target):
    if listed(source, target, RETURN_BY_LINE):
        return None
    mirrored = (LINE - 1 - source, LINE - 1 - target)
    if (source, target) in ADDERS:
        adder = ADDERS[(source, target)]
    elif mirrored in ADDERS:
        adder = LINE - 1 - ADDERS[mirrored]
    else:
        return None
    return None if listed(adder, target, RETURN_BY_LINE) else adder


def silu(v):
    return v / (1.0 + jnp.exp(-v))


def fused_kernel(
    sp,
    tp,
    q_hbm,
    k_hbm,
    v_hbm,
    sink_hbm,
    wo_hbm,
    res_hbm,
    gain_hbm,
    routes_hbm,
    gw_hbm,
    eg_hbm,
    eu_hbm,
    ed_hbm,
    sg_hbm,
    su_hbm,
    sd_hbm,
    out_ref,
    q_v,
    k_v,
    v_v,
    sink_s,
    wo_v,
    res_v,
    gain_v,
    routes_v,
    gw_v,
    eg_v,
    eu_v,
    ed_v,
    sg_v,
    su_v,
    sd_v,
    eg_o,
    eu_o,
    ed_o,
    sg_o,
    su_o,
    sd_o,
    halo_k,
    halo_v,
    att_v,
    proj,
    psend,
    precv,
    pxs,
    pxr,
    pys,
    pyr,
    stream_v,
    mirror_v,
    tail_s,
    tail_m,
    nrm,
    part,
    xsend,
    xrecv,
    zsend,
    zrecv,
    zadd,
    load_sem,
    halo_r,
    pr_sem,
    w_s,
    w_r,
    send_sem,
    nrm_r,
    xr_sem,
    zr_sem,
    za_sem,
    far_sem,
):
    z = lax.axis_index("sp")
    t = lax.axis_index("tp")
    c = t % PAIR
    x = t // PAIR
    t_core = x * PAIR + (1 - c)
    t_x = (1 - x) * PAIR + c
    core = {"tp": t_core}
    xnbr = {"tp": t_x}
    upper = z // (sp // 2)

    def at_z(pos):
        return {"sp": pos}

    def rcopy(src, dst, ssem, rsem, dev):
        return pltpu.make_async_remote_copy(
            src_ref=src,
            dst_ref=dst,
            send_sem=ssem,
            recv_sem=rsem,
            device_id=dev,
            device_id_type=pl.DeviceIdType.MESH,
        )

    def signal(sem, dev):
        pl.semaphore_signal(sem, inc=1, device_id=dev, device_id_type=pl.DeviceIdType.MESH)

    moves = [
        (k_hbm, k_v),
        (v_hbm, v_v),
        (q_hbm, q_v),
        (sink_hbm, sink_s),
        (routes_hbm, routes_v),
        (gw_hbm, gw_v),
        (wo_hbm, wo_v),
        (res_hbm, res_v),
        (gain_hbm, gain_v),
        (sg_hbm, sg_v),
        (su_hbm, su_v),
        (sd_hbm, sd_v),
        (eg_hbm.at[0], eg_v),
        (eu_hbm.at[0], eu_v),
        (ed_hbm.at[0], ed_v),
    ]
    early = 9
    loads = [
        pltpu.make_async_copy(a, b, load_sem.at[i if i < early else i - early])
        for i, (a, b) in enumerate(moves)
    ]
    pending = []

    def sent(copy, condition=None):
        pending.append((copy, condition))

    def slot():
        if len(pending) >= SENDS:
            settle(len(pending) - SENDS)
        return send_sem.at[len(pending) % SENDS]

    def settle(index):
        copy, condition = pending[index]
        if copy is None:
            return
        pending[index] = (None, None)
        if condition is None:
            copy.wait_send()
        else:
            pl.when(condition)(copy.wait_send)

    barrier = pltpu.get_barrier_semaphore()
    for dev in (core, xnbr):
        signal(barrier, dev)

    @pl.when(z > 0)
    def _():
        signal(barrier, at_z(z - 1))

    @pl.when(z < sp - 1)
    def _():
        signal(barrier, at_z(z + 1))

    for load in loads[:early]:
        load.start()
    rows = stream_v.shape[0]
    width = stream_v.shape[1]
    length = q_v.shape[0]
    heads = q_v.shape[1] // HEAD
    kv_heads = k_v.shape[1] // HEAD
    grouped = heads // kv_heads

    @pl.when(z == 0)
    def _():
        halo_k[0] = jnp.zeros(halo_k.shape[1:], halo_k.dtype)
        halo_v[0] = jnp.zeros(halo_v.shape[1:], halo_v.dtype)

    @pl.when(z == sp - 1)
    def _():
        halo_k[1] = jnp.zeros(halo_k.shape[1:], halo_k.dtype)
        halo_v[1] = jnp.zeros(halo_v.shape[1:], halo_v.dtype)

    loads[0].wait()
    loads[1].wait()
    peers = 2 + jnp.where(z > 0, 1, 0) + jnp.where(z < sp - 1, 1, 0)
    pl.semaphore_wait(barrier, peers)

    def halo(up, which, sem):
        pos = z + 1 if up else z - 1
        row = 0 if up else 1
        src = (k_v, v_v)[which]
        dst = (halo_k, halo_v)[which]
        return rcopy(src, dst.at[row], sem, halo_r.at[row, which], at_z(pos))

    def halo_wait(row, which):
        src = (k_v, v_v)[which]
        dst = (halo_k, halo_v)[which]
        rcopy(src, dst.at[row], send_sem.at[0], halo_r.at[row, which], core).wait_recv()

    for which in range(2):
        for up, condition in ((True, z < sp - 1), (False, z > 0)):
            copy = halo(up, which, slot())
            pl.when(condition)(copy.start)
            sent(copy, condition)

    def push(i, src, dst):
        return rcopy(src, dst, w_s.at[i], w_r.at[i], core)

    pushes = [
        push(0, eg_hbm.at[0], eg_o),
        push(1, sg_hbm, sg_o),
        push(2, su_hbm, su_o),
        push(3, sd_hbm, sd_o),
        push(4, eu_hbm.at[0], eu_o),
        push(5, ed_hbm.at[0], ed_o),
    ]
    for copy in pushes[:2]:
        copy.start()

    for k in range(2, 6):
        loads[k].wait()
    for load in loads[early:]:
        load.start()
    half = LANES // 2
    lane = lax.broadcasted_iota(jnp.int32, (rows, LANES), 1)
    unit = lax.broadcasted_iota(jnp.int32, (LANES, rows), 0)
    unit = jnp.where(unit < half, unit, unit - half)
    combine = jnp.zeros((LANES, rows), jnp.float32)
    for k in range(TOPK):
        combine = combine + jnp.where(routes_v[k : k + 1] == unit, gw_v[k : k + 1], 0.0)
    combine = combine.T
    high = combine.astype(jnp.bfloat16)
    low = (combine - high.astype(jnp.float32)).astype(jnp.bfloat16)
    own_tail = jnp.where(
        lane < half, high.astype(jnp.float32), low.astype(jnp.float32)
    ).astype(jnp.bfloat16)
    nrm[z, x, :, width:] = own_tail
    tail_s[...] = own_tail
    tail_copy = rcopy(tail_s, tail_m, slot(), w_r.at[6], xnbr)
    tail_copy.start()
    sent(tail_copy)

    contract = (((1,), (1,)), ((), ()))
    scale = HEAD ** (-0.5)

    def cols(head):
        return slice(head * HEAD, (head + 1) * HEAD)

    def stacked(kv):
        first = kv * grouped
        return jnp.concatenate(
            [q_v[:, cols(first + i)] for i in range(grouped)], axis=0
        ) * jnp.asarray(scale, q_v.dtype)

    def product(a, b):
        return lax.dot_general(a, b, contract, preferred_element_type=jnp.float32)

    queries = [stacked(kv) for kv in range(kv_heads)]
    row = lax.broadcasted_iota(jnp.int32, (grouped * length, 1), 0)
    tops = []
    sums = []
    outs = []
    for kv in range(kv_heads):
        scores = product(queries[kv], k_v[:, cols(kv)])
        sink = jnp.full((grouped * length, 1), sink_s[kv * grouped], jnp.float32)
        for i in range(1, grouped):
            sink = jnp.where(row >= i * length, sink_s[kv * grouped + i], sink)
        top = jnp.maximum(jnp.max(scores, axis=-1, keepdims=True), sink)
        e = jnp.exp(scores - top)
        tops.append(top)
        sums.append(jnp.exp(sink - top) + jnp.sum(e, axis=-1, keepdims=True))
        outs.append(
            jnp.dot(e.astype(jnp.bfloat16), v_v[:, cols(kv)], preferred_element_type=jnp.float32)
        )

    qi = lax.broadcasted_iota(jnp.int32, (grouped * length, length), 0) % length
    ki = lax.broadcasted_iota(jnp.int32, (grouped * length, length), 1)
    low_bound = jnp.where(z > 0, 0, length)
    high_bound = jnp.where(z < sp - 1, 0, length)
    low_mask = ki - qi >= low_bound
    high_mask = qi - ki >= high_bound

    def wait_halo(which):
        @pl.when(z > 0)
        def _():
            halo_wait(0, which)

        @pl.when(z < sp - 1)
        def _():
            halo_wait(1, which)

    wait_halo(0)
    sides = []
    for kv in range(kv_heads):
        s_low = jnp.where(low_mask, product(queries[kv], halo_k[0, :, cols(kv)]), -jnp.inf)
        s_high = jnp.where(high_mask, product(queries[kv], halo_k[1, :, cols(kv)]), -jnp.inf)
        top = jnp.max(jnp.maximum(s_low, s_high), axis=-1, keepdims=True)
        top = jnp.maximum(top, tops[kv])
        e_low = jnp.exp(s_low - top)
        e_high = jnp.exp(s_high - top)
        shrink = jnp.exp(tops[kv] - top)
        denominator = shrink * sums[kv] + jnp.sum(e_low + e_high, axis=-1, keepdims=True)
        sides.append(
            (
                shrink * outs[kv],
                e_low.astype(jnp.bfloat16),
                e_high.astype(jnp.bfloat16),
                1.0 / denominator,
            )
        )
    wait_halo(1)
    for kv in range(kv_heads):
        base, e_low, e_high, inverse = sides[kv]
        base = base + jnp.dot(
            e_low, halo_v[0, :, cols(kv)], preferred_element_type=jnp.float32
        )
        base = base + jnp.dot(
            e_high, halo_v[1, :, cols(kv)], preferred_element_type=jnp.float32
        )
        base = (base * inverse).astype(jnp.bfloat16)
        for i in range(grouped):
            att_v[:, :, cols(kv * grouped + i)] = base[i * length : (i + 1) * length].reshape(
                tp, rows, HEAD
            )

    @pl.when(z == 1)
    def _():
        signal(far_sem, at_z(z - 1))

    @pl.when(z == sp - 2)
    def _():
        signal(far_sem, at_z(z + 1))

    loads[6].wait()

    def projected(cc):
        picked = jnp.concatenate([att_v[xh * PAIR + cc] for xh in range(PAIR)], axis=0)
        return jnp.dot(picked, wo_v[...], preferred_element_type=jnp.float32)

    psend[...] = projected(1 - c).astype(jnp.bfloat16).reshape(psend.shape)
    pcore = []
    for order, xx in enumerate((1 - x, x)):
        pcore.append(rcopy(psend.at[xx], precv.at[xx], slot(), pr_sem.at[order], core))
        pcore[-1].start()
        sent(pcore[-1])
    for copy in pushes[2:]:
        copy.start()
    proj[...] = projected(c).reshape(proj.shape)
    piece = rows // CHUNKS

    def cut(j):
        return pl.ds(j * piece, piece)

    def cross(src, dst, k):
        copy = rcopy(src, dst, slot(), pr_sem.at[PAIR + k], xnbr)
        copy.start()
        sent(copy)
        return copy

    pcore[0].wait_recv()
    mirror_v[...] = proj[1 - x] + precv[1 - x].astype(jnp.float32)
    pcross = []
    for j in range(CHUNKS):
        pxs[cut(j)] = mirror_v[cut(j)].astype(jnp.bfloat16)
        pcross.append(cross(pxs.at[cut(j)], pxr.at[cut(j)], j))
    loads[7].wait()
    loads[8].wait()
    pcore[1].wait_recv()
    stream_v[...] = res_v[...].astype(jnp.float32) + proj[x] + precv[x].astype(jnp.float32)
    pmirror = []
    for j in range(CHUNKS):
        pys[cut(j)] = stream_v[cut(j)].astype(jnp.bfloat16)
        pmirror.append(cross(pys.at[cut(j)], pyr.at[cut(j)], CHUNKS + j))
    tail_copy.wait_recv()
    nrm[z, 1 - x, :, width:] = tail_m[...]

    def normalized(stream):
        return (
            stream
            * lax.rsqrt(jnp.mean(stream * stream, axis=-1, keepdims=True) + norm_eps)
            * gain_v[...]
        ).astype(jnp.bfloat16)

    expert = z * tp + t
    sibling = z * tp + t_core

    def schedule(me):
        def place(p):
            return p + upper * (sp - 1 - 2 * p)

        def send(src, dst, rsem, dev):
            copy = rcopy(src, dst, slot(), rsem, dev)
            copy.start()
            sent(copy)

        def side(h):
            return x if h == "o" else 1 - x

        def block_send(p, h, j, dev):
            g = place(p)
            ref = nrm.at[g, side(h), cut(j)]
            send(ref, ref, nrm_r.at[g, side(h), j], dev)

        def block_wait(p, h, j):
            g = place(p)
            ref = nrm.at[g, side(h), cut(j)]
            rcopy(ref, ref, send_sem.at[0], nrm_r.at[g, side(h), j], core).wait_recv()

        def cross_copy(p, j, sem):
            g = place(p)
            return rcopy(
                xsend.at[g, cut(j)], xrecv.at[g, cut(j)], sem, xr_sem.at[g, j], xnbr
            )

        lane_of = {"o": 0, "m": 1}

        def line_send(p, h, span):
            g = place(p)
            send(
                zsend.at[g, side(h), span],
                zrecv.at[z, side(h), span],
                zr_sem.at[z, lane_of[h]],
                at_z(g),
            )

        def line_wait(p, h):
            g = place(p)
            ref = zrecv.at[g, side(h)]
            rcopy(ref, ref, send_sem.at[0], zr_sem.at[g, lane_of[h]], core).wait_recv()
            return zrecv[g, side(h)].astype(jnp.float32)

        def add_send(p, j, adder):
            g = place(p)
            send(
                zsend.at[g, x, cut(j)], zadd.at[g, cut(j)], za_sem.at[g, j], at_z(place(adder))
            )

        def add_wait(p, j):
            g = place(p)
            ref = zadd.at[g, cut(j)]
            rcopy(ref, ref, send_sem.at[0], za_sem.at[g, j], core).wait_recv()
            return zadd[g, cut(j)].astype(jnp.float32)

        def cross_wait(p, j):
            cross_copy(p, j, send_sem.at[0]).wait_recv()
            g = place(p)
            return part[g, x, cut(j)] + xrecv[g, cut(j)].astype(jnp.float32)

        waited = set()

        def once(name, copies):
            if name not in waited:
                waited.add(name)
                for copy in copies:
                    copy()

        def own_weights():
            once("own", [loads[k].wait for k in range(9, 15)])

        def sibling_experts():
            once("experts", [pushes[k].wait_recv for k in (0, 4, 5)])

        def sibling_shared():
            once("shared", [pushes[k].wait_recv for k in (1, 2, 3)])

        def one(acts, gate_ref, up_ref, down_ref):
            gate = jnp.dot(acts, gate_ref[...], preferred_element_type=jnp.float32)
            up = jnp.dot(acts, up_ref[...], preferred_element_type=jnp.float32)
            hidden = (silu(gate) * up).astype(jnp.bfloat16)
            out = jnp.dot(hidden, down_ref[...], preferred_element_type=jnp.float32)
            return out.astype(jnp.bfloat16).astype(jnp.float32)

        def rows_of(places):
            block = [nrm[g].reshape(PAIR * rows, nrm.shape[-1]) for g in places]
            block = jnp.concatenate(block * 2 if len(block) == 1 else block, axis=0)
            return block[:, :width], block[:, width:].astype(jnp.float32)

        def weight(tail, e):
            lanes = lax.broadcasted_iota(jnp.int32, tail.shape, 1)
            mine = (lanes == e) | (lanes == e + half)
            return jnp.sum(jnp.where(mine, tail, 0.0), axis=-1, keepdims=True)

        def experts(ps):
            own_weights()
            sibling_experts()
            places = [place(p) for p in ps]
            acts, tail = rows_of(places)
            result = weight(tail, expert) * one(acts, eg_v, eu_v, ed_v)
            result = result + weight(tail, sibling) * one(acts, eg_o, eu_o, ed_o)
            result = result[: len(ps) * PAIR * rows].reshape(len(ps), PAIR, rows, width)
            for i, g in enumerate(places):
                part[g] = result[i]

        own_parts = [op for op in ORDER[me] if op[0] == "Q"]

        def own_part(op):
            own_weights()
            acts, tail = rows_of([z])
            if op[1] == 0:
                result = weight(tail, expert) * one(acts, eg_v, eu_v, ed_v)
            elif op[1] == 1:
                sibling_experts()
                result = weight(tail, sibling) * one(acts, eg_o, eu_o, ed_o)
            else:
                sibling_shared()
                result = one(acts, sg_v, su_v, sd_v) + one(acts, sg_o, su_o, sd_o)
            result = result[: PAIR * rows].reshape(PAIR, rows, width)
            if op == own_parts[0]:
                part[z] = result
            else:
                part[z] = part[z] + result

        knows_far = False
        summed = set()
        tail_from = None
        for op in ORDER[me]:
            kind = op[0]
            if kind == "E" and tail_from is None:
                tail_from = len(pending)
            if kind in "HG" and not summed:
                for index in range(tail_from):
                    settle(index)
                for copy in pushes:
                    copy.wait_send()
                summed.add(me)
            with jax.named_scope("op_" + "_".join(str(v) for v in op)):
                if kind == "N":
                    j = op[1]
                    pcross[j].wait_recv()
                    stream = stream_v[cut(j)] + pxr[cut(j)].astype(jnp.float32)
                    stream_v[cut(j)] = stream
                    nrm[z, x, cut(j), :width] = normalized(stream)
                elif kind == "M":
                    j = op[1]
                    pmirror[j].wait_recv()
                    stream = mirror_v[cut(j)] + pyr[cut(j)].astype(jnp.float32)
                    nrm[z, 1 - x, cut(j), :width] = normalized(stream)
                elif kind == "S":
                    h, p, j = op[1:]
                    if relay_of(me, p) is None and (
                        h == "o" or listed(me, p, DISPATCH_BY_LINE)
                    ):
                        if me == 0 and p == LINE - 1 and not knows_far:
                            pl.semaphore_wait(far_sem, 1)
                            knows_far = True
                        block_send(me, h, j, at_z(place(p)))
                elif kind == "A":
                    p, h, j = op[1:]
                    block_wait(p, h, j)
                    mirrored_in = listed(p, me, DISPATCH_BY_LINE)
                    if h == "o" and not mirrored_in:
                        block_send(p, h, j, xnbr)
                    for q in range(LINE):
                        if q not in (p, me) and relay_of(p, q) == me:
                            if h == "o" or (mirrored_in and listed(p, q, DISPATCH_BY_LINE)):
                                block_send(p, h, j, at_z(place(q)))
                elif kind == "D":
                    experts(op[1])
                elif kind == "Q":
                    own_part(op)
                elif kind == "E":
                    p = op[1]
                    g = place(p)
                    if p != me and listed(me, p, RETURN_BY_LINE):
                        for h in ("o", "m"):
                            zsend[g, side(h)] = part[g, side(h)].astype(jnp.bfloat16)
                            line_send(p, h, slice(None))
                    else:
                        if p == me:
                            for q in range(LINE):
                                if q != me and listed(q, me, RETURN_BY_LINE):
                                    part[g, 1 - x] = part[g, 1 - x] + line_wait(q, "m")
                        for j in range(CHUNKS):
                            xsend[g, cut(j)] = part[g, 1 - x, cut(j)].astype(jnp.bfloat16)
                            copy = cross_copy(p, j, slot())
                            copy.start()
                            sent(copy)
                elif kind == "F":
                    p, j = op[1:]
                    if not listed(me, p, RETURN_BY_LINE):
                        value = cross_wait(p, j)
                        for q in range(LINE):
                            if q not in (p, me) and adder_of(q, p) == me:
                                value = value + add_wait(p, j)
                        zsend[place(p), x, cut(j)] = value.astype(jnp.bfloat16)
                        adder = adder_of(me, p)
                        if adder is None:
                            line_send(p, "o", cut(j))
                        else:
                            add_send(p, j, adder)
                elif kind == "H":
                    j = op[1]
                    stream_v[cut(j)] = stream_v[cut(j)] + cross_wait(me, j)
                elif kind == "G":
                    p = op[1]
                    last = [other for other in ORDER[me] if other[:2] == ("G", p)][-1]
                    if op == last and adder_of(p, me) is None:
                        stream_v[...] = stream_v[...] + line_wait(p, "o")
        out_ref[...] = stream_v[...].astype(out_ref.dtype)
        if me == 0 and not knows_far:
            pl.semaphore_wait(far_sem, 1)
        with jax.named_scope("lastwaits"):
            for index in range(len(pending)):
                settle(index)

    shared_pending = list(pending)
    for me in range(LINE // 2):

        @pl.when((z == me) | (z == sp - 1 - me))
        def _():
            pending[:] = shared_pending
            schedule(me)


def fused_scratch(sp, tp, shapes):
    (q, k, v, sink, wo, res, gain, routes, gw, eg, eu, ed, sg, su, sd) = shapes
    rows, width = res.shape
    bf = jnp.bfloat16
    f32 = jnp.float32
    return [
        (q.shape, bf),
        (k.shape, bf),
        (v.shape, bf),
        (sink.shape, f32),
        (wo.shape, bf),
        (res.shape, bf),
        (gain.shape, f32),
        (routes.shape, jnp.int32),
        (gw.shape, f32),
        (eg.shape[1:], bf),
        (eu.shape[1:], bf),
        (ed.shape[1:], bf),
        (sg.shape, bf),
        (su.shape, bf),
        (sd.shape, bf),
        (eg.shape[1:], bf),
        (eu.shape[1:], bf),
        (ed.shape[1:], bf),
        (sg.shape, bf),
        (su.shape, bf),
        (sd.shape, bf),
        ((2,) + k.shape, bf),
        ((2,) + v.shape, bf),
        ((tp, rows, q.shape[1]), bf),
        ((PAIR, rows, width), f32),
        ((PAIR, rows, width), bf),
        ((PAIR, rows, width), bf),
        ((rows, width), bf),
        ((rows, width), bf),
        ((rows, width), bf),
        ((rows, width), bf),
        ((rows, width), f32),
        ((rows, width), f32),
        ((rows, LANES), bf),
        ((rows, LANES), bf),
        ((sp, PAIR, rows, width + LANES), bf),
        ((sp, PAIR, rows, width), f32),
        ((sp, rows, width), bf),
        ((sp, rows, width), bf),
        ((sp, PAIR, rows, width), bf),
        ((sp, PAIR, rows, width), bf),
        ((sp, rows, width), bf),
    ]


def size_of(shape, dtype):
    total = jnp.dtype(dtype).itemsize
    for extent in shape:
        total *= extent
    return total


def fused(sp, tp, buffers, *args):
    dma = pltpu.SemaphoreType.DMA
    res = args[5]
    scratch = [pltpu.VMEM(s, d) for s, d in buffers]
    scratch[3] = pltpu.SMEM(*buffers[3])
    return pl.pallas_call(
        functools.partial(fused_kernel, sp, tp),
        out_shape=pltpu.VMEM(res.shape, jnp.bfloat16),
        in_specs=[pl.BlockSpec(memory_space=pltpu.HBM)] * 15,
        out_specs=pl.BlockSpec(memory_space=pltpu.VMEM),
        scratch_shapes=scratch
        + [
            dma((9,)),
            dma((2, 2)),
            dma((PAIR + 2 * CHUNKS,)),
            dma((6,)),
            dma((7,)),
            dma((SENDS,)),
            dma((sp, PAIR, CHUNKS)),
            dma((sp, CHUNKS)),
            dma((sp, PAIR)),
            dma((sp, CHUNKS)),
            pltpu.SemaphoreType.REGULAR,
        ],
        compiler_params=pltpu.CompilerParams(
            collective_id=0, has_side_effects=True, vmem_limit_bytes=VMEM_BYTES
        ),
    )(*args)


def either(*args):
    sp = lax.axis_size("sp")
    tp = lax.axis_size("tp")
    args = list(args)
    shaped = list(args)
    shaped[6] = args[6].reshape(1, -1)
    shaped[7] = args[7].T
    shaped[8] = args[8].T
    buffers = fused_scratch(sp, tp, shaped)
    needed = sum(size_of(s, d) for s, d in buffers)
    fits = (
        2 * needed <= VMEM_BYTES
        and tp == 2 * PAIR
        and sp == LINE
        and args[5].shape[0] % (16 * CHUNKS) == 0
        and 2 * sp * tp <= LANES
        and args[0].shape[0] == WINDOW
        and args[9].shape[0] == 1
    )
    if fits:
        return fused(sp, tp, buffers, *shaped)
    return body(*args)


def solution(mesh):
    placed = (
        P(("grp", "sp"), "tp"),
        P(("grp", "sp"), "tp"),
        P(("grp", "sp"), "tp"),
        P("tp"),
        P("tp", None),
        P(("grp", "sp", "tp"), None),
        P(),
        P(("grp", "sp", "tp"), None),
        P(("grp", "sp", "tp"), None),
        P(("sp", "tp"), None, None),
        P(("sp", "tp"), None, None),
        P(("sp", "tp"), None, None),
        P(None, "tp"),
        P(None, "tp"),
        P("tp", None),
    )
    return jax.shard_map(
        either, mesh=mesh, in_specs=placed, out_specs=P(("grp", "sp", "tp"), None), check_vma=False
    )
```

```python
import functools

import jax
import jax.numpy as jnp
from jax import lax
from jax.experimental import pallas as pl
from jax.experimental.pallas import tpu as pltpu
from jax.sharding import PartitionSpec as P

HEAD = 64
WINDOW = 128
TOPK = 6


norm_eps = 1e-06


def with_halo(block, sides, width):
    for axis, dim in sides:
        count = lax.axis_size(axis)
        forward = [(i, i + 1) for i in range(count - 1)]
        backward = [(target, source) for source, target in forward]
        low = lax.ppermute(
            lax.slice_in_dim(block, block.shape[dim] - width, None, axis=dim), axis, forward
        )
        high = lax.ppermute(lax.slice_in_dim(block, 0, width, axis=dim), axis, backward)
        block = jnp.concatenate([low, block, high], axis=dim)
    return block


def window_attention(query_rows, key_rows, value_rows, sink_logit):
    local_len = query_rows.shape[0]
    head_size = HEAD
    local_kv = key_rows.shape[1] // head_size
    local_heads = query_rows.shape[1] // head_size
    grouped = local_heads // local_kv
    blocks = local_len // WINDOW
    stacked = jnp.stack([key_rows, value_rows])
    widened = with_halo(stacked, (("sp", 1),), WINDOW)
    banded = widened.reshape(2, blocks + 2, WINDOW, local_kv, head_size)
    banded = jnp.concatenate([banded[:, :-2], banded[:, 1:-1], banded[:, 2:]], axis=2)
    queries = query_rows.reshape(blocks, WINDOW, local_kv, grouped, head_size)
    scores = jnp.einsum(
        "nqhgd,nkhd->nhgqk", queries, banded[0], preferred_element_type=jnp.float32
    ) * head_size ** (-0.5)
    seq_start = lax.axis_index("sp") * local_len
    total_len = lax.axis_size("sp") * local_len
    block_ids = jnp.arange(blocks, dtype=jnp.int32)[:, None, None]
    query_pos = seq_start + block_ids * WINDOW + jnp.arange(WINDOW, dtype=jnp.int32)[None, :, None]
    key_pos = (
        seq_start
        + (block_ids - 1) * WINDOW
        + jnp.arange(3 * WINDOW, dtype=jnp.int32)[None, None, :]
    )
    in_window = (jnp.abs(key_pos - query_pos) <= WINDOW) & (key_pos >= 0) & (key_pos < total_len)
    scores = jnp.where(in_window[:, None, None], scores, -jnp.inf)
    sink_part = sink_logit.reshape(1, local_kv, grouped, 1, 1)
    row_max = jnp.maximum(sink_part, jnp.max(scores, axis=-1, keepdims=True))
    shifted = jnp.exp(scores - row_max)
    denominator = jnp.exp(sink_part - row_max) + jnp.sum(shifted, axis=-1, keepdims=True)
    weights = (shifted / denominator).astype(jnp.bfloat16)
    attended = jnp.einsum(
        "nhgqk,nkhd->nqhgd", weights, banded[1], preferred_element_type=jnp.float32
    )
    return attended.astype(jnp.bfloat16).reshape(local_len, local_heads * head_size)


def body(
    query_rows,
    key_rows,
    value_rows,
    sink_logit,
    out_weight,
    residual,
    norm_gain,
    routes,
    gate_weights,
    expert_gate,
    expert_up,
    expert_down,
    shared_gate,
    shared_up,
    shared_down,
):
    attended = window_attention(query_rows, key_rows, value_rows, sink_logit)
    tok_dev = attended.shape[0]
    tok_rows = residual.shape[0]
    model_width = residual.shape[1]
    projected = lax.psum_scatter(
        jnp.dot(attended, out_weight, preferred_element_type=jnp.float32).astype(jnp.bfloat16),
        "tp",
        scatter_dimension=0,
        tiled=True,
    ).astype(jnp.float32)
    stream = residual.astype(jnp.float32) + projected
    normed = (
        stream * lax.rsqrt(jnp.mean(stream * stream, axis=-1, keepdims=True) + norm_eps) * norm_gain
    ).astype(jnp.bfloat16)
    sp_count = lax.axis_size("sp")
    tp_count = lax.axis_size("tp")
    experts_all = sp_count * tp_count
    capacity = (2 * tok_dev * TOPK + tp_count * experts_all - 1) // (tp_count * experts_all)
    copies = tok_rows * TOPK
    flat_expert = routes.reshape(-1)
    one_hot = (flat_expert[:, None] == jnp.arange(experts_all, dtype=jnp.int32)[None, :]).astype(
        jnp.int32
    )
    rank_in_expert = jnp.sum(jnp.cumsum(one_hot, axis=0) * one_hot, axis=1) - 1
    target_slot = flat_expert * capacity + rank_in_expert
    slot_token = (
        jnp.full((experts_all * capacity,), tok_rows, jnp.int32)
        .at[target_slot]
        .set(jnp.arange(copies, dtype=jnp.int32) // TOPK)
    )
    padded_rows = jnp.concatenate([normed, jnp.zeros((1, model_width), jnp.bfloat16)], axis=0)
    outgoing = padded_rows[slot_token].reshape(experts_all, capacity, model_width)
    incoming = lax.all_to_all(outgoing, ("sp", "tp"), split_axis=0, concat_axis=0, tiled=True)
    shaped = incoming.reshape(-1, model_width)
    gate_part = jnp.dot(shaped, expert_gate[0], preferred_element_type=jnp.float32)
    up_part = jnp.dot(shaped, expert_up[0], preferred_element_type=jnp.float32)
    hidden = (jax.nn.silu(gate_part) * up_part).astype(jnp.bfloat16)
    result = jnp.dot(hidden, expert_down[0], preferred_element_type=jnp.float32).astype(
        jnp.bfloat16
    )
    returned = lax.all_to_all(
        result.reshape(incoming.shape), ("sp", "tp"), split_axis=0, concat_axis=0, tiled=True
    )
    returned = returned.reshape(experts_all * capacity, model_width)
    gathered_copies = returned[target_slot].reshape(tok_rows, TOPK, model_width)
    routed = jnp.sum(gate_weights[:, :, None] * gathered_copies.astype(jnp.float32), axis=1)
    slab_rows = lax.all_gather(normed, "tp", axis=0, tiled=True)
    gate_part = jnp.dot(slab_rows, shared_gate, preferred_element_type=jnp.float32)
    up_part = jnp.dot(slab_rows, shared_up, preferred_element_type=jnp.float32)
    hidden = (jax.nn.silu(gate_part) * up_part).astype(jnp.bfloat16)
    partials = jnp.dot(hidden, shared_down, preferred_element_type=jnp.float32)
    shared = lax.psum_scatter(
        partials.astype(jnp.bfloat16), "tp", scatter_dimension=0, tiled=True
    ).astype(jnp.float32)
    return (stream + routed + shared).astype(jnp.bfloat16)


VMEM_BYTES = 66 * 1000 * 1000
PAIR = 2
LINE = 4
LANES = 128
CHUNKS = 2
SENDS = 20
DISPATCH_BY_LINE = ((1, 2),)
RETURN_BY_LINE = ((0, 1), (1, 3),)
RELAYS = {(0, 2): 1, (0, 3): 2, (1, 3): 2}
ADDERS = {(0, 2): 1, (1, 3): 2}
ORDER = {
    0: (
        ("N", 0),
        ("S", "o", 1, 0),
        ("N", 1),
        ("S", "o", 1, 1),
        ("A", 1, "o", 0),
        ("M", 0),
        ("S", "o", 2, 0),
        ("A", 1, "o", 1),
        ("M", 1),
        ("Q", 2),
        ("Q", 1),
        ("A", 2, "o", 0),
        ("S", "m", 2, 1),
        ("A", 1, "m", 0),
        ("A", 2, "o", 1),
        ("A", 1, "m", 1),
        ("D", (1,)),
        ("A", 3, "o", 0),
        ("A", 2, "m", 0),
        ("A", 3, "o", 1),
        ("E", 1),
        ("A", 2, "m", 1),
        ("D", (2,)),
        ("E", 2),
        ("S", "o", 3, 0),
        ("A", 3, "m", 0),
        ("A", 3, "m", 1),
        ("F", 1, 1),
        ("D", (3,)),
        ("S", "o", 2, 1),
        ("E", 3),
        ("F", 2, 1),
        ("S", "m", 3, 1),
        ("F", 2, 0),
        ("Q", 0),
        ("S", "o", 3, 1),
        ("G", 2, 0),
        ("F", 3, 0),
        ("S", "m", 1, 0),
        ("F", 3, 1),
        ("F", 1, 0),
        ("E", 0),
        ("H", 0),
        ("G", 3, 0),
        ("S", "m", 1, 1),
        ("G", 2, 1),
        ("H", 1),
        ("G", 1, 0),
        ("S", "m", 2, 0),
        ("G", 1, 1),
        ("G", 3, 1),
        ("S", "m", 3, 0),
    ),
    1: (
        ("N", 0),
        ("S", "o", 2, 0),
        ("S", "o", 0, 0),
        ("N", 1),
        ("S", "o", 2, 1),
        ("S", "o", 0, 1),
        ("M", 0),
        ("A", 0, "o", 0),
        ("A", 2, "o", 0),
        ("M", 1),
        ("A", 0, "o", 1),
        ("G", 3, 0),
        ("A", 2, "o", 1),
        ("A", 3, "o", 0),
        ("S", "m", 2, 1),
        ("Q", 1),
        ("A", 0, "m", 1),
        ("A", 3, "o", 1),
        ("A", 2, "m", 1),
        ("Q", 2),
        ("A", 0, "m", 0),
        ("S", "o", 3, 1),
        ("S", "m", 2, 0),
        ("A", 3, "m", 0),
        ("A", 3, "m", 1),
        ("D", (3,)),
        ("E", 3),
        ("A", 2, "m", 0),
        ("D", (0, 2)),
        ("E", 2),
        ("G", 3, 1),
        ("Q", 0),
        ("S", "m", 0, 1),
        ("E", 0),
        ("F", 2, 1),
        ("F", 0, 0),
        ("F", 3, 1),
        ("G", 0, 0),
        ("F", 0, 1),
        ("S", "m", 3, 0),
        ("F", 2, 0),
        ("G", 0, 1),
        ("S", "m", 0, 0),
        ("E", 1),
        ("S", "o", 3, 0),
        ("F", 3, 0),
        ("S", "m", 3, 1),
        ("G", 2, 0),
        ("G", 2, 1),
        ("H", 0),
        ("H", 1),
    ),
}


def listed(source, target, pairs):
    mirrored = (LINE - 1 - source, LINE - 1 - target)
    return (source, target) in pairs or mirrored in pairs


def relay_of(source, target):
    if (source, target) in RELAYS:
        return RELAYS[(source, target)]
    mirrored = (LINE - 1 - source, LINE - 1 - target)
    if mirrored in RELAYS:
        return LINE - 1 - RELAYS[mirrored]
    return None


def adder_of(source, target):
    if listed(source, target, RETURN_BY_LINE):
        return None
    mirrored = (LINE - 1 - source, LINE - 1 - target)
    if (source, target) in ADDERS:
        adder = ADDERS[(source, target)]
    elif mirrored in ADDERS:
        adder = LINE - 1 - ADDERS[mirrored]
    else:
        return None
    return None if listed(adder, target, RETURN_BY_LINE) else adder


def silu(v):
    return v / (1.0 + jnp.exp(-v))


def fused_kernel(
    sp,
    tp,
    q_hbm,
    k_hbm,
    v_hbm,
    sink_hbm,
    wo_hbm,
    res_hbm,
    gain_hbm,
    routes_hbm,
    gw_hbm,
    eg_hbm,
    eu_hbm,
    ed_hbm,
    sg_hbm,
    su_hbm,
    sd_hbm,
    out_ref,
    q_v,
    k_v,
    v_v,
    sink_s,
    wo_v,
    res_v,
    gain_v,
    routes_v,
    gw_v,
    eg_v,
    eu_v,
    ed_v,
    sg_v,
    su_v,
    sd_v,
    eg_o,
    eu_o,
    ed_o,
    sg_o,
    su_o,
    sd_o,
    halo_k,
    halo_v,
    att_v,
    proj,
    psend,
    precv,
    pxs,
    pxr,
    pys,
    pyr,
    stream_v,
    mirror_v,
    tail_s,
    tail_m,
    nrm,
    part,
    xsend,
    xrecv,
    zsend,
    zrecv,
    zadd,
    load_sem,
    halo_r,
    pr_sem,
    w_s,
    w_r,
    send_sem,
    nrm_r,
    xr_sem,
    zr_sem,
    za_sem,
    far_sem,
):
    z = lax.axis_index("sp")
    t = lax.axis_index("tp")
    c = t % PAIR
    x = t // PAIR
    t_core = x * PAIR + (1 - c)
    t_x = (1 - x) * PAIR + c
    core = {"tp": t_core}
    xnbr = {"tp": t_x}
    upper = z // (sp // 2)

    def at_z(pos):
        return {"sp": pos}

    def rcopy(src, dst, ssem, rsem, dev):
        return pltpu.make_async_remote_copy(
            src_ref=src,
            dst_ref=dst,
            send_sem=ssem,
            recv_sem=rsem,
            device_id=dev,
            device_id_type=pl.DeviceIdType.MESH,
        )

    def signal(sem, dev):
        pl.semaphore_signal(sem, inc=1, device_id=dev, device_id_type=pl.DeviceIdType.MESH)

    moves = [
        (k_hbm, k_v),
        (v_hbm, v_v),
        (q_hbm, q_v),
        (sink_hbm, sink_s),
        (routes_hbm, routes_v),
        (gw_hbm, gw_v),
        (wo_hbm, wo_v),
        (res_hbm, res_v),
        (gain_hbm, gain_v),
        (sg_hbm, sg_v),
        (su_hbm, su_v),
        (sd_hbm, sd_v),
        (eg_hbm.at[0], eg_v),
        (eu_hbm.at[0], eu_v),
        (ed_hbm.at[0], ed_v),
    ]
    early = 9
    loads = [
        pltpu.make_async_copy(a, b, load_sem.at[i if i < early else i - early])
        for i, (a, b) in enumerate(moves)
    ]
    pending = []

    def sent(copy, condition=None):
        pending.append((copy, condition))

    def slot():
        if len(pending) >= SENDS:
            settle(len(pending) - SENDS)
        return send_sem.at[len(pending) % SENDS]

    def settle(index):
        copy, condition = pending[index]
        if copy is None:
            return
        pending[index] = (None, None)
        if condition is None:
            copy.wait_send()
        else:
            pl.when(condition)(copy.wait_send)

    barrier = pltpu.get_barrier_semaphore()
    for dev in (core, xnbr):
        signal(barrier, dev)

    @pl.when(z > 0)
    def _():
        signal(barrier, at_z(z - 1))

    @pl.when(z < sp - 1)
    def _():
        signal(barrier, at_z(z + 1))

    for load in loads[:early]:
        load.start()
    rows = stream_v.shape[0]
    width = stream_v.shape[1]
    length = q_v.shape[0]
    heads = q_v.shape[1] // HEAD
    kv_heads = k_v.shape[1] // HEAD
    grouped = heads // kv_heads

    @pl.when(z == 0)
    def _():
        halo_k[0] = jnp.zeros(halo_k.shape[1:], halo_k.dtype)
        halo_v[0] = jnp.zeros(halo_v.shape[1:], halo_v.dtype)

    @pl.when(z == sp - 1)
    def _():
        halo_k[1] = jnp.zeros(halo_k.shape[1:], halo_k.dtype)
        halo_v[1] = jnp.zeros(halo_v.shape[1:], halo_v.dtype)

    loads[0].wait()
    loads[1].wait()
    peers = 2 + jnp.where(z > 0, 1, 0) + jnp.where(z < sp - 1, 1, 0)
    pl.semaphore_wait(barrier, peers)

    def halo(up, which, sem):
        pos = z + 1 if up else z - 1
        row = 0 if up else 1
        src = (k_v, v_v)[which]
        dst = (halo_k, halo_v)[which]
        return rcopy(src, dst.at[row], sem, halo_r.at[row, which], at_z(pos))

    def halo_wait(row, which):
        src = (k_v, v_v)[which]
        dst = (halo_k, halo_v)[which]
        rcopy(src, dst.at[row], send_sem.at[0], halo_r.at[row, which], core).wait_recv()

    for which in range(2):
        for up, condition in ((True, z < sp - 1), (False, z > 0)):
            copy = halo(up, which, slot())
            pl.when(condition)(copy.start)
            sent(copy, condition)

    def push(i, src, dst):
        return rcopy(src, dst, w_s.at[i], w_r.at[i], core)

    pushes = [
        push(0, eg_hbm.at[0], eg_o),
        push(1, sg_hbm, sg_o),
        push(2, su_hbm, su_o),
        push(3, sd_hbm, sd_o),
        push(4, eu_hbm.at[0], eu_o),
        push(5, ed_hbm.at[0], ed_o),
    ]
    for copy in pushes[:2]:
        copy.start()

    for k in range(2, 6):
        loads[k].wait()
    for load in loads[early:]:
        load.start()
    half = LANES // 2
    lane = lax.broadcasted_iota(jnp.int32, (rows, LANES), 1)
    unit = lax.broadcasted_iota(jnp.int32, (LANES, rows), 0)
    unit = jnp.where(unit < half, unit, unit - half)
    combine = jnp.zeros((LANES, rows), jnp.float32)
    for k in range(TOPK):
        combine = combine + jnp.where(routes_v[k : k + 1] == unit, gw_v[k : k + 1], 0.0)
    combine = combine.T
    high = combine.astype(jnp.bfloat16)
    low = (combine - high.astype(jnp.float32)).astype(jnp.bfloat16)
    own_tail = jnp.where(
        lane < half, high.astype(jnp.float32), low.astype(jnp.float32)
    ).astype(jnp.bfloat16)
    nrm[z, x, :, width:] = own_tail
    tail_s[...] = own_tail
    tail_copy = rcopy(tail_s, tail_m, slot(), w_r.at[6], xnbr)
    tail_copy.start()
    sent(tail_copy)

    contract = (((1,), (1,)), ((), ()))
    scale = HEAD ** (-0.5)

    def cols(head):
        return slice(head * HEAD, (head + 1) * HEAD)

    def stacked(kv):
        first = kv * grouped
        return jnp.concatenate(
            [q_v[:, cols(first + i)] for i in range(grouped)], axis=0
        ) * jnp.asarray(scale, q_v.dtype)

    def product(a, b):
        return lax.dot_general(a, b, contract, preferred_element_type=jnp.float32)

    queries = [stacked(kv) for kv in range(kv_heads)]
    row = lax.broadcasted_iota(jnp.int32, (grouped * length, 1), 0)
    tops = []
    sums = []
    outs = []
    for kv in range(kv_heads):
        scores = product(queries[kv], k_v[:, cols(kv)])
        sink = jnp.full((grouped * length, 1), sink_s[kv * grouped], jnp.float32)
        for i in range(1, grouped):
            sink = jnp.where(row >= i * length, sink_s[kv * grouped + i], sink)
        top = jnp.maximum(jnp.max(scores, axis=-1, keepdims=True), sink)
        e = jnp.exp(scores - top)
        tops.append(top)
        sums.append(jnp.exp(sink - top) + jnp.sum(e, axis=-1, keepdims=True))
        outs.append(
            jnp.dot(e.astype(jnp.bfloat16), v_v[:, cols(kv)], preferred_element_type=jnp.float32)
        )

    qi = lax.broadcasted_iota(jnp.int32, (grouped * length, length), 0) % length
    ki = lax.broadcasted_iota(jnp.int32, (grouped * length, length), 1)
    low_bound = jnp.where(z > 0, 0, length)
    high_bound = jnp.where(z < sp - 1, 0, length)
    low_mask = ki - qi >= low_bound
    high_mask = qi - ki >= high_bound

    def wait_halo(which):
        @pl.when(z > 0)
        def _():
            halo_wait(0, which)

        @pl.when(z < sp - 1)
        def _():
            halo_wait(1, which)

    wait_halo(0)
    sides = []
    for kv in range(kv_heads):
        s_low = jnp.where(low_mask, product(queries[kv], halo_k[0, :, cols(kv)]), -jnp.inf)
        s_high = jnp.where(high_mask, product(queries[kv], halo_k[1, :, cols(kv)]), -jnp.inf)
        top = jnp.max(jnp.maximum(s_low, s_high), axis=-1, keepdims=True)
        top = jnp.maximum(top, tops[kv])
        e_low = jnp.exp(s_low - top)
        e_high = jnp.exp(s_high - top)
        shrink = jnp.exp(tops[kv] - top)
        denominator = shrink * sums[kv] + jnp.sum(e_low + e_high, axis=-1, keepdims=True)
        sides.append(
            (
                shrink * outs[kv],
                e_low.astype(jnp.bfloat16),
                e_high.astype(jnp.bfloat16),
                1.0 / denominator,
            )
        )
    wait_halo(1)
    for kv in range(kv_heads):
        base, e_low, e_high, inverse = sides[kv]
        base = base + jnp.dot(
            e_low, halo_v[0, :, cols(kv)], preferred_element_type=jnp.float32
        )
        base = base + jnp.dot(
            e_high, halo_v[1, :, cols(kv)], preferred_element_type=jnp.float32
        )
        base = (base * inverse).astype(jnp.bfloat16)
        for i in range(grouped):
            att_v[:, :, cols(kv * grouped + i)] = base[i * length : (i + 1) * length].reshape(
                tp, rows, HEAD
            )

    @pl.when(z == 1)
    def _():
        signal(far_sem, at_z(z - 1))

    @pl.when(z == sp - 2)
    def _():
        signal(far_sem, at_z(z + 1))

    loads[6].wait()

    def projected(cc):
        picked = jnp.concatenate([att_v[xh * PAIR + cc] for xh in range(PAIR)], axis=0)
        return jnp.dot(picked, wo_v[...], preferred_element_type=jnp.float32)

    psend[...] = projected(1 - c).astype(jnp.bfloat16).reshape(psend.shape)
    pcore = []
    for order, xx in enumerate((1 - x, x)):
        pcore.append(rcopy(psend.at[xx], precv.at[xx], slot(), pr_sem.at[order], core))
        pcore[-1].start()
        sent(pcore[-1])
    for copy in pushes[2:]:
        copy.start()
    proj[...] = projected(c).reshape(proj.shape)
    piece = rows // CHUNKS

    def cut(j):
        return pl.ds(j * piece, piece)

    def cross(src, dst, k):
        copy = rcopy(src, dst, slot(), pr_sem.at[PAIR + k], xnbr)
        copy.start()
        sent(copy)
        return copy

    pcore[0].wait_recv()
    mirror_v[...] = proj[1 - x] + precv[1 - x].astype(jnp.float32)
    pcross = []
    for j in range(CHUNKS):
        pxs[cut(j)] = mirror_v[cut(j)].astype(jnp.bfloat16)
        pcross.append(cross(pxs.at[cut(j)], pxr.at[cut(j)], j))
    loads[7].wait()
    loads[8].wait()
    pcore[1].wait_recv()
    stream_v[...] = res_v[...].astype(jnp.float32) + proj[x] + precv[x].astype(jnp.float32)
    pmirror = []
    for j in range(CHUNKS):
        pys[cut(j)] = stream_v[cut(j)].astype(jnp.bfloat16)
        pmirror.append(cross(pys.at[cut(j)], pyr.at[cut(j)], CHUNKS + j))
    tail_copy.wait_recv()
    nrm[z, 1 - x, :, width:] = tail_m[...]

    def normalized(stream):
        return (
            stream
            * lax.rsqrt(jnp.mean(stream * stream, axis=-1, keepdims=True) + norm_eps)
            * gain_v[...]
        ).astype(jnp.bfloat16)

    expert = z * tp + t
    sibling = z * tp + t_core

    def schedule(me):
        def place(p):
            return p + upper * (sp - 1 - 2 * p)

        def send(src, dst, rsem, dev):
            copy = rcopy(src, dst, slot(), rsem, dev)
            copy.start()
            sent(copy)

        def side(h):
            return x if h == "o" else 1 - x

        def block_send(p, h, j, dev):
            g = place(p)
            ref = nrm.at[g, side(h), cut(j)]
            send(ref, ref, nrm_r.at[g, side(h), j], dev)

        def block_wait(p, h, j):
            g = place(p)
            ref = nrm.at[g, side(h), cut(j)]
            rcopy(ref, ref, send_sem.at[0], nrm_r.at[g, side(h), j], core).wait_recv()

        def cross_copy(p, j, sem):
            g = place(p)
            return rcopy(
                xsend.at[g, cut(j)], xrecv.at[g, cut(j)], sem, xr_sem.at[g, j], xnbr
            )

        lane_of = {"o": 0, "m": 1}

        def line_send(p, h, span):
            g = place(p)
            send(
                zsend.at[g, side(h), span],
                zrecv.at[z, side(h), span],
                zr_sem.at[z, lane_of[h]],
                at_z(g),
            )

        def line_wait(p, h):
            g = place(p)
            ref = zrecv.at[g, side(h)]
            rcopy(ref, ref, send_sem.at[0], zr_sem.at[g, lane_of[h]], core).wait_recv()
            return zrecv[g, side(h)].astype(jnp.float32)

        def add_send(p, j, adder):
            g = place(p)
            send(
                zsend.at[g, x, cut(j)], zadd.at[g, cut(j)], za_sem.at[g, j], at_z(place(adder))
            )

        def add_wait(p, j):
            g = place(p)
            ref = zadd.at[g, cut(j)]
            rcopy(ref, ref, send_sem.at[0], za_sem.at[g, j], core).wait_recv()
            return zadd[g, cut(j)].astype(jnp.float32)

        def cross_wait(p, j):
            cross_copy(p, j, send_sem.at[0]).wait_recv()
            g = place(p)
            return part[g, x, cut(j)] + xrecv[g, cut(j)].astype(jnp.float32)

        waited = set()

        def once(name, copies):
            if name not in waited:
                waited.add(name)
                for copy in copies:
                    copy()

        def own_weights():
            once("own", [loads[k].wait for k in range(9, 15)])

        def sibling_experts():
            once("experts", [pushes[k].wait_recv for k in (0, 4, 5)])

        def sibling_shared():
            once("shared", [pushes[k].wait_recv for k in (1, 2, 3)])

        def one(acts, gate_ref, up_ref, down_ref):
            gate = jnp.dot(acts, gate_ref[...], preferred_element_type=jnp.float32)
            up = jnp.dot(acts, up_ref[...], preferred_element_type=jnp.float32)
            hidden = (silu(gate) * up).astype(jnp.bfloat16)
            out = jnp.dot(hidden, down_ref[...], preferred_element_type=jnp.float32)
            return out.astype(jnp.bfloat16).astype(jnp.float32)

        def rows_of(places):
            block = [nrm[g].reshape(PAIR * rows, nrm.shape[-1]) for g in places]
            block = jnp.concatenate(block * 2 if len(block) == 1 else block, axis=0)
            return block[:, :width], block[:, width:].astype(jnp.float32)

        def weight(tail, e):
            lanes = lax.broadcasted_iota(jnp.int32, tail.shape, 1)
            mine = (lanes == e) | (lanes == e + half)
            return jnp.sum(jnp.where(mine, tail, 0.0), axis=-1, keepdims=True)

        def experts(ps):
            own_weights()
            sibling_experts()
            places = [place(p) for p in ps]
            acts, tail = rows_of(places)
            result = weight(tail, expert) * one(acts, eg_v, eu_v, ed_v)
            result = result + weight(tail, sibling) * one(acts, eg_o, eu_o, ed_o)
            result = result[: len(ps) * PAIR * rows].reshape(len(ps), PAIR, rows, width)
            for i, g in enumerate(places):
                part[g] = result[i]

        own_parts = [op for op in ORDER[me] if op[0] == "Q"]

        def own_part(op):
            own_weights()
            acts, tail = rows_of([z])
            if op[1] == 0:
                result = weight(tail, expert) * one(acts, eg_v, eu_v, ed_v)
            elif op[1] == 1:
                sibling_experts()
                result = weight(tail, sibling) * one(acts, eg_o, eu_o, ed_o)
            else:
                sibling_shared()
                result = one(acts, sg_v, su_v, sd_v) + one(acts, sg_o, su_o, sd_o)
            result = result[: PAIR * rows].reshape(PAIR, rows, width)
            if op == own_parts[0]:
                part[z] = result
            else:
                part[z] = part[z] + result

        knows_far = False
        summed = set()
        tail_from = None
        for op in ORDER[me]:
            kind = op[0]
            if kind == "E" and tail_from is None:
                tail_from = len(pending)
            if kind in "HG" and tail_from is not None and not summed:
                for index in range(tail_from):
                    settle(index)
                for copy in pushes:
                    copy.wait_send()
                summed.add(me)
            with jax.named_scope("op_" + "_".join(str(v) for v in op)):
                if kind == "N":
                    j = op[1]
                    pcross[j].wait_recv()
                    stream = stream_v[cut(j)] + pxr[cut(j)].astype(jnp.float32)
                    stream_v[cut(j)] = stream
                    nrm[z, x, cut(j), :width] = normalized(stream)
                elif kind == "M":
                    j = op[1]
                    pmirror[j].wait_recv()
                    stream = mirror_v[cut(j)] + pyr[cut(j)].astype(jnp.float32)
                    nrm[z, 1 - x, cut(j), :width] = normalized(stream)
                elif kind == "S":
                    h, p, j = op[1:]
                    if relay_of(me, p) is None and (
                        h == "o" or listed(me, p, DISPATCH_BY_LINE)
                    ):
                        if me == 0 and p == LINE - 1 and not knows_far:
                            pl.semaphore_wait(far_sem, 1)
                            knows_far = True
                        block_send(me, h, j, at_z(place(p)))
                elif kind == "A":
                    p, h, j = op[1:]
                    block_wait(p, h, j)
                    mirrored_in = listed(p, me, DISPATCH_BY_LINE)
                    if h == "o" and not mirrored_in:
                        block_send(p, h, j, xnbr)
                    for q in range(LINE):
                        if q not in (p, me) and relay_of(p, q) == me:
                            if h == "o" or (mirrored_in and listed(p, q, DISPATCH_BY_LINE)):
                                block_send(p, h, j, at_z(place(q)))
                elif kind == "D":
                    experts(op[1])
                elif kind == "Q":
                    own_part(op)
                elif kind == "E":
                    p = op[1]
                    g = place(p)
                    if p != me and listed(me, p, RETURN_BY_LINE):
                        for h in ("o", "m"):
                            zsend[g, side(h)] = part[g, side(h)].astype(jnp.bfloat16)
                            line_send(p, h, slice(None))
                    else:
                        if p == me:
                            for q in range(LINE):
                                if q != me and listed(q, me, RETURN_BY_LINE):
                                    part[g, 1 - x] = part[g, 1 - x] + line_wait(q, "m")
                        for j in range(CHUNKS):
                            xsend[g, cut(j)] = part[g, 1 - x, cut(j)].astype(jnp.bfloat16)
                            copy = cross_copy(p, j, slot())
                            copy.start()
                            sent(copy)
                elif kind == "F":
                    p, j = op[1:]
                    if not listed(me, p, RETURN_BY_LINE):
                        value = cross_wait(p, j)
                        for q in range(LINE):
                            if q not in (p, me) and adder_of(q, p) == me:
                                value = value + add_wait(p, j)
                        zsend[place(p), x, cut(j)] = value.astype(jnp.bfloat16)
                        adder = adder_of(me, p)
                        if adder is None:
                            line_send(p, "o", cut(j))
                        else:
                            add_send(p, j, adder)
                elif kind == "H":
                    j = op[1]
                    stream_v[cut(j)] = stream_v[cut(j)] + cross_wait(me, j)
                elif kind == "G":
                    p = op[1]
                    last = [other for other in ORDER[me] if other[:2] == ("G", p)][-1]
                    if op == last and adder_of(p, me) is None:
                        stream_v[...] = stream_v[...] + line_wait(p, "o")
        out_ref[...] = stream_v[...].astype(out_ref.dtype)
        if me == 0 and not knows_far:
            pl.semaphore_wait(far_sem, 1)
        with jax.named_scope("lastwaits"):
            for index in range(len(pending)):
                settle(index)

    shared_pending = list(pending)
    for me in range(LINE // 2):

        @pl.when((z == me) | (z == sp - 1 - me))
        def _():
            pending[:] = shared_pending
            schedule(me)


def fused_scratch(sp, tp, shapes):
    (q, k, v, sink, wo, res, gain, routes, gw, eg, eu, ed, sg, su, sd) = shapes
    rows, width = res.shape
    bf = jnp.bfloat16
    f32 = jnp.float32
    return [
        (q.shape, bf),
        (k.shape, bf),
        (v.shape, bf),
        (sink.shape, f32),
        (wo.shape, bf),
        (res.shape, bf),
        (gain.shape, f32),
        (routes.shape, jnp.int32),
        (gw.shape, f32),
        (eg.shape[1:], bf),
        (eu.shape[1:], bf),
        (ed.shape[1:], bf),
        (sg.shape, bf),
        (su.shape, bf),
        (sd.shape, bf),
        (eg.shape[1:], bf),
        (eu.shape[1:], bf),
        (ed.shape[1:], bf),
        (sg.shape, bf),
        (su.shape, bf),
        (sd.shape, bf),
        ((2,) + k.shape, bf),
        ((2,) + v.shape, bf),
        ((tp, rows, q.shape[1]), bf),
        ((PAIR, rows, width), f32),
        ((PAIR, rows, width), bf),
        ((PAIR, rows, width), bf),
        ((rows, width), bf),
        ((rows, width), bf),
        ((rows, width), bf),
        ((rows, width), bf),
        ((rows, width), f32),
        ((rows, width), f32),
        ((rows, LANES), bf),
        ((rows, LANES), bf),
        ((sp, PAIR, rows, width + LANES), bf),
        ((sp, PAIR, rows, width), f32),
        ((sp, rows, width), bf),
        ((sp, rows, width), bf),
        ((sp, PAIR, rows, width), bf),
        ((sp, PAIR, rows, width), bf),
        ((sp, rows, width), bf),
    ]


def size_of(shape, dtype):
    total = jnp.dtype(dtype).itemsize
    for extent in shape:
        total *= extent
    return total


def fused(sp, tp, buffers, *args):
    dma = pltpu.SemaphoreType.DMA
    res = args[5]
    scratch = [pltpu.VMEM(s, d) for s, d in buffers]
    scratch[3] = pltpu.SMEM(*buffers[3])
    return pl.pallas_call(
        functools.partial(fused_kernel, sp, tp),
        out_shape=pltpu.VMEM(res.shape, jnp.bfloat16),
        in_specs=[pl.BlockSpec(memory_space=pltpu.HBM)] * 15,
        out_specs=pl.BlockSpec(memory_space=pltpu.VMEM),
        scratch_shapes=scratch
        + [
            dma((9,)),
            dma((2, 2)),
            dma((PAIR + 2 * CHUNKS,)),
            dma((6,)),
            dma((7,)),
            dma((SENDS,)),
            dma((sp, PAIR, CHUNKS)),
            dma((sp, CHUNKS)),
            dma((sp, PAIR)),
            dma((sp, CHUNKS)),
            pltpu.SemaphoreType.REGULAR,
        ],
        compiler_params=pltpu.CompilerParams(
            collective_id=0, has_side_effects=True, vmem_limit_bytes=VMEM_BYTES
        ),
    )(*args)


def either(*args):
    sp = lax.axis_size("sp")
    tp = lax.axis_size("tp")
    args = list(args)
    shaped = list(args)
    shaped[6] = args[6].reshape(1, -1)
    shaped[7] = args[7].T
    shaped[8] = args[8].T
    buffers = fused_scratch(sp, tp, shaped)
    needed = sum(size_of(s, d) for s, d in buffers)
    fits = (
        2 * needed <= VMEM_BYTES
        and tp == 2 * PAIR
        and sp == LINE
        and args[5].shape[0] % (16 * CHUNKS) == 0
        and 2 * sp * tp <= LANES
        and args[0].shape[0] == WINDOW
        and args[9].shape[0] == 1
    )
    if fits:
        return fused(sp, tp, buffers, *shaped)
    return body(*args)


def solution(mesh):
    placed = (
        P(("grp", "sp"), "tp"),
        P(("grp", "sp"), "tp"),
        P(("grp", "sp"), "tp"),
        P("tp"),
        P("tp", None),
        P(("grp", "sp", "tp"), None),
        P(),
        P(("grp", "sp", "tp"), None),
        P(("grp", "sp", "tp"), None),
        P(("sp", "tp"), None, None),
        P(("sp", "tp"), None, None),
        P(("sp", "tp"), None, None),
        P(None, "tp"),
        P(None, "tp"),
        P("tp", None),
    )
    return jax.shard_map(
        either, mesh=mesh, in_specs=placed, out_specs=P(("grp", "sp", "tp"), None), check_vma=False
    )
```

```python
import functools

import jax
import jax.numpy as jnp
from jax import lax
from jax.experimental import pallas as pl
from jax.experimental.pallas import tpu as pltpu
from jax.sharding import PartitionSpec as P

HEAD = 64
WINDOW = 128
TOPK = 6


norm_eps = 1e-06


def with_halo(block, sides, width):
    for axis, dim in sides:
        count = lax.axis_size(axis)
        forward = [(i, i + 1) for i in range(count - 1)]
        backward = [(target, source) for source, target in forward]
        low = lax.ppermute(
            lax.slice_in_dim(block, block.shape[dim] - width, None, axis=dim), axis, forward
        )
        high = lax.ppermute(lax.slice_in_dim(block, 0, width, axis=dim), axis, backward)
        block = jnp.concatenate([low, block, high], axis=dim)
    return block


def window_attention(query_rows, key_rows, value_rows, sink_logit):
    local_len = query_rows.shape[0]
    head_size = HEAD
    local_kv = key_rows.shape[1] // head_size
    local_heads = query_rows.shape[1] // head_size
    grouped = local_heads // local_kv
    blocks = local_len // WINDOW
    stacked = jnp.stack([key_rows, value_rows])
    widened = with_halo(stacked, (("sp", 1),), WINDOW)
    banded = widened.reshape(2, blocks + 2, WINDOW, local_kv, head_size)
    banded = jnp.concatenate([banded[:, :-2], banded[:, 1:-1], banded[:, 2:]], axis=2)
    queries = query_rows.reshape(blocks, WINDOW, local_kv, grouped, head_size)
    scores = jnp.einsum(
        "nqhgd,nkhd->nhgqk", queries, banded[0], preferred_element_type=jnp.float32
    ) * head_size ** (-0.5)
    seq_start = lax.axis_index("sp") * local_len
    total_len = lax.axis_size("sp") * local_len
    block_ids = jnp.arange(blocks, dtype=jnp.int32)[:, None, None]
    query_pos = seq_start + block_ids * WINDOW + jnp.arange(WINDOW, dtype=jnp.int32)[None, :, None]
    key_pos = (
        seq_start
        + (block_ids - 1) * WINDOW
        + jnp.arange(3 * WINDOW, dtype=jnp.int32)[None, None, :]
    )
    in_window = (jnp.abs(key_pos - query_pos) <= WINDOW) & (key_pos >= 0) & (key_pos < total_len)
    scores = jnp.where(in_window[:, None, None], scores, -jnp.inf)
    sink_part = sink_logit.reshape(1, local_kv, grouped, 1, 1)
    row_max = jnp.maximum(sink_part, jnp.max(scores, axis=-1, keepdims=True))
    shifted = jnp.exp(scores - row_max)
    denominator = jnp.exp(sink_part - row_max) + jnp.sum(shifted, axis=-1, keepdims=True)
    weights = (shifted / denominator).astype(jnp.bfloat16)
    attended = jnp.einsum(
        "nhgqk,nkhd->nqhgd", weights, banded[1], preferred_element_type=jnp.float32
    )
    return attended.astype(jnp.bfloat16).reshape(local_len, local_heads * head_size)


def body(
    query_rows,
    key_rows,
    value_rows,
    sink_logit,
    out_weight,
    residual,
    norm_gain,
    routes,
    gate_weights,
    expert_gate,
    expert_up,
    expert_down,
    shared_gate,
    shared_up,
    shared_down,
):
    attended = window_attention(query_rows, key_rows, value_rows, sink_logit)
    tok_dev = attended.shape[0]
    tok_rows = residual.shape[0]
    model_width = residual.shape[1]
    projected = lax.psum_scatter(
        jnp.dot(attended, out_weight, preferred_element_type=jnp.float32).astype(jnp.bfloat16),
        "tp",
        scatter_dimension=0,
        tiled=True,
    ).astype(jnp.float32)
    stream = residual.astype(jnp.float32) + projected
    normed = (
        stream * lax.rsqrt(jnp.mean(stream * stream, axis=-1, keepdims=True) + norm_eps) * norm_gain
    ).astype(jnp.bfloat16)
    sp_count = lax.axis_size("sp")
    tp_count = lax.axis_size("tp")
    experts_all = sp_count * tp_count
    capacity = (2 * tok_dev * TOPK + tp_count * experts_all - 1) // (tp_count * experts_all)
    copies = tok_rows * TOPK
    flat_expert = routes.reshape(-1)
    one_hot = (flat_expert[:, None] == jnp.arange(experts_all, dtype=jnp.int32)[None, :]).astype(
        jnp.int32
    )
    rank_in_expert = jnp.sum(jnp.cumsum(one_hot, axis=0) * one_hot, axis=1) - 1
    target_slot = flat_expert * capacity + rank_in_expert
    slot_token = (
        jnp.full((experts_all * capacity,), tok_rows, jnp.int32)
        .at[target_slot]
        .set(jnp.arange(copies, dtype=jnp.int32) // TOPK)
    )
    padded_rows = jnp.concatenate([normed, jnp.zeros((1, model_width), jnp.bfloat16)], axis=0)
    outgoing = padded_rows[slot_token].reshape(experts_all, capacity, model_width)
    incoming = lax.all_to_all(outgoing, ("sp", "tp"), split_axis=0, concat_axis=0, tiled=True)
    shaped = incoming.reshape(-1, model_width)
    gate_part = jnp.dot(shaped, expert_gate[0], preferred_element_type=jnp.float32)
    up_part = jnp.dot(shaped, expert_up[0], preferred_element_type=jnp.float32)
    hidden = (jax.nn.silu(gate_part) * up_part).astype(jnp.bfloat16)
    result = jnp.dot(hidden, expert_down[0], preferred_element_type=jnp.float32).astype(
        jnp.bfloat16
    )
    returned = lax.all_to_all(
        result.reshape(incoming.shape), ("sp", "tp"), split_axis=0, concat_axis=0, tiled=True
    )
    returned = returned.reshape(experts_all * capacity, model_width)
    gathered_copies = returned[target_slot].reshape(tok_rows, TOPK, model_width)
    routed = jnp.sum(gate_weights[:, :, None] * gathered_copies.astype(jnp.float32), axis=1)
    slab_rows = lax.all_gather(normed, "tp", axis=0, tiled=True)
    gate_part = jnp.dot(slab_rows, shared_gate, preferred_element_type=jnp.float32)
    up_part = jnp.dot(slab_rows, shared_up, preferred_element_type=jnp.float32)
    hidden = (jax.nn.silu(gate_part) * up_part).astype(jnp.bfloat16)
    partials = jnp.dot(hidden, shared_down, preferred_element_type=jnp.float32)
    shared = lax.psum_scatter(
        partials.astype(jnp.bfloat16), "tp", scatter_dimension=0, tiled=True
    ).astype(jnp.float32)
    return (stream + routed + shared).astype(jnp.bfloat16)


VMEM_BYTES = 66 * 1000 * 1000
PAIR = 2
LINE = 4
LANES = 128
CHUNKS = 2
SENDS = 20
DISPATCH_BY_LINE = ((1, 2),)
RETURN_BY_LINE = ((0, 1), (1, 3),)
RELAYS = {(0, 2): 1, (0, 3): 2, (1, 3): 2}
ADDERS = {(0, 2): 1, (1, 3): 2}
ORDER = {
    0: (
        ("N", 0),
        ("S", "o", 1, 0),
        ("N", 1),
        ("S", "o", 1, 1),
        ("A", 1, "o", 0),
        ("M", 0),
        ("S", "o", 2, 0),
        ("A", 1, "o", 1),
        ("M", 1),
        ("Q", 2),
        ("Q", 1),
        ("A", 2, "o", 0),
        ("S", "m", 2, 1),
        ("A", 1, "m", 0),
        ("A", 2, "o", 1),
        ("A", 1, "m", 1),
        ("D", (1,)),
        ("A", 3, "o", 0),
        ("A", 2, "m", 0),
        ("A", 3, "o", 1),
        ("E", 1),
        ("A", 2, "m", 1),
        ("D", (2,)),
        ("E", 2),
        ("S", "o", 3, 0),
        ("A", 3, "m", 0),
        ("A", 3, "m", 1),
        ("F", 1, 1),
        ("D", (3,)),
        ("S", "o", 2, 1),
        ("E", 3),
        ("F", 2, 1),
        ("S", "m", 3, 1),
        ("F", 2, 0),
        ("Q", 0),
        ("S", "o", 3, 1),
        ("G", 2, 0),
        ("F", 3, 0),
        ("S", "m", 1, 0),
        ("F", 3, 1),
        ("F", 1, 0),
        ("E", 0),
        ("H", 0),
        ("G", 3, 0),
        ("S", "m", 1, 1),
        ("G", 2, 1),
        ("H", 1),
        ("G", 1, 0),
        ("S", "m", 2, 0),
        ("G", 1, 1),
        ("G", 3, 1),
        ("S", "m", 3, 0),
    ),
    1: (
        ("N", 0),
        ("S", "o", 2, 0),
        ("S", "o", 0, 0),
        ("N", 1),
        ("S", "o", 2, 1),
        ("S", "o", 0, 1),
        ("M", 0),
        ("A", 0, "o", 0),
        ("A", 2, "o", 0),
        ("M", 1),
        ("A", 0, "o", 1),
        ("G", 3, 0),
        ("A", 2, "o", 1),
        ("A", 3, "o", 0),
        ("S", "m", 2, 1),
        ("Q", 1),
        ("A", 0, "m", 1),
        ("A", 3, "o", 1),
        ("A", 2, "m", 1),
        ("Q", 2),
        ("A", 0, "m", 0),
        ("S", "o", 3, 1),
        ("S", "m", 2, 0),
        ("A", 3, "m", 0),
        ("A", 3, "m", 1),
        ("D", (3,)),
        ("E", 3),
        ("A", 2, "m", 0),
        ("D", (0, 2)),
        ("E", 2),
        ("E", 0),
        ("G", 3, 1),
        ("Q", 0),
        ("S", "m", 0, 1),
        ("F", 0, 0),
        ("F", 0, 1),
        ("F", 2, 1),
        ("F", 3, 1),
        ("G", 0, 0),
        ("S", "m", 3, 0),
        ("F", 2, 0),
        ("G", 0, 1),
        ("S", "m", 0, 0),
        ("E", 1),
        ("S", "o", 3, 0),
        ("F", 3, 0),
        ("S", "m", 3, 1),
        ("G", 2, 0),
        ("G", 2, 1),
        ("H", 0),
        ("H", 1),
    ),
}


def listed(source, target, pairs):
    mirrored = (LINE - 1 - source, LINE - 1 - target)
    return (source, target) in pairs or mirrored in pairs


def relay_of(source, target):
    if (source, target) in RELAYS:
        return RELAYS[(source, target)]
    mirrored = (LINE - 1 - source, LINE - 1 - target)
    if mirrored in RELAYS:
        return LINE - 1 - RELAYS[mirrored]
    return None


def adder_of(source, target):
    if listed(source, target, RETURN_BY_LINE):
        return None
    mirrored = (LINE - 1 - source, LINE - 1 - target)
    if (source, target) in ADDERS:
        adder = ADDERS[(source, target)]
    elif mirrored in ADDERS:
        adder = LINE - 1 - ADDERS[mirrored]
    else:
        return None
    return None if listed(adder, target, RETURN_BY_LINE) else adder


def silu(v):
    return v / (1.0 + jnp.exp(-v))


def fused_kernel(
    sp,
    tp,
    q_hbm,
    k_hbm,
    v_hbm,
    sink_hbm,
    wo_hbm,
    res_hbm,
    gain_hbm,
    routes_hbm,
    gw_hbm,
    eg_hbm,
    eu_hbm,
    ed_hbm,
    sg_hbm,
    su_hbm,
    sd_hbm,
    out_ref,
    q_v,
    k_v,
    v_v,
    sink_s,
    wo_v,
    res_v,
    gain_v,
    routes_v,
    gw_v,
    eg_v,
    eu_v,
    ed_v,
    sg_v,
    su_v,
    sd_v,
    eg_o,
    eu_o,
    ed_o,
    sg_o,
    su_o,
    sd_o,
    halo_k,
    halo_v,
    att_v,
    proj,
    psend,
    precv,
    pxs,
    pxr,
    pys,
    pyr,
    stream_v,
    mirror_v,
    tail_s,
    tail_m,
    nrm,
    part,
    xsend,
    xrecv,
    zsend,
    zrecv,
    zadd,
    load_sem,
    halo_r,
    pr_sem,
    w_s,
    w_r,
    send_sem,
    nrm_r,
    xr_sem,
    zr_sem,
    za_sem,
    far_sem,
):
    z = lax.axis_index("sp")
    t = lax.axis_index("tp")
    c = t % PAIR
    x = t // PAIR
    t_core = x * PAIR + (1 - c)
    t_x = (1 - x) * PAIR + c
    core = {"tp": t_core}
    xnbr = {"tp": t_x}
    upper = z // (sp // 2)

    def at_z(pos):
        return {"sp": pos}

    def rcopy(src, dst, ssem, rsem, dev):
        return pltpu.make_async_remote_copy(
            src_ref=src,
            dst_ref=dst,
            send_sem=ssem,
            recv_sem=rsem,
            device_id=dev,
            device_id_type=pl.DeviceIdType.MESH,
        )

    def signal(sem, dev):
        pl.semaphore_signal(sem, inc=1, device_id=dev, device_id_type=pl.DeviceIdType.MESH)

    moves = [
        (k_hbm, k_v),
        (v_hbm, v_v),
        (q_hbm, q_v),
        (sink_hbm, sink_s),
        (routes_hbm, routes_v),
        (gw_hbm, gw_v),
        (wo_hbm, wo_v),
        (res_hbm, res_v),
        (gain_hbm, gain_v),
        (sg_hbm, sg_v),
        (su_hbm, su_v),
        (sd_hbm, sd_v),
        (eg_hbm.at[0], eg_v),
        (eu_hbm.at[0], eu_v),
        (ed_hbm.at[0], ed_v),
    ]
    early = 9
    loads = [
        pltpu.make_async_copy(a, b, load_sem.at[i if i < early else i - early])
        for i, (a, b) in enumerate(moves)
    ]
    pending = []

    def sent(copy, condition=None):
        pending.append((copy, condition))

    def slot():
        if len(pending) >= SENDS:
            settle(len(pending) - SENDS)
        return send_sem.at[len(pending) % SENDS]

    def settle(index):
        copy, condition = pending[index]
        if copy is None:
            return
        pending[index] = (None, None)
        if condition is None:
            copy.wait_send()
        else:
            pl.when(condition)(copy.wait_send)

    barrier = pltpu.get_barrier_semaphore()
    for dev in (core, xnbr):
        signal(barrier, dev)

    @pl.when(z > 0)
    def _():
        signal(barrier, at_z(z - 1))

    @pl.when(z < sp - 1)
    def _():
        signal(barrier, at_z(z + 1))

    for load in loads[:early]:
        load.start()
    rows = stream_v.shape[0]
    width = stream_v.shape[1]
    length = q_v.shape[0]
    heads = q_v.shape[1] // HEAD
    kv_heads = k_v.shape[1] // HEAD
    grouped = heads // kv_heads

    @pl.when(z == 0)
    def _():
        halo_k[0] = jnp.zeros(halo_k.shape[1:], halo_k.dtype)
        halo_v[0] = jnp.zeros(halo_v.shape[1:], halo_v.dtype)

    @pl.when(z == sp - 1)
    def _():
        halo_k[1] = jnp.zeros(halo_k.shape[1:], halo_k.dtype)
        halo_v[1] = jnp.zeros(halo_v.shape[1:], halo_v.dtype)

    loads[0].wait()
    loads[1].wait()
    peers = 2 + jnp.where(z > 0, 1, 0) + jnp.where(z < sp - 1, 1, 0)
    pl.semaphore_wait(barrier, peers)

    def halo(up, which, sem):
        pos = z + 1 if up else z - 1
        row = 0 if up else 1
        src = (k_v, v_v)[which]
        dst = (halo_k, halo_v)[which]
        return rcopy(src, dst.at[row], sem, halo_r.at[row, which], at_z(pos))

    def halo_wait(row, which):
        src = (k_v, v_v)[which]
        dst = (halo_k, halo_v)[which]
        rcopy(src, dst.at[row], send_sem.at[0], halo_r.at[row, which], core).wait_recv()

    for which in range(2):
        for up, condition in ((True, z < sp - 1), (False, z > 0)):
            copy = halo(up, which, slot())
            pl.when(condition)(copy.start)
            sent(copy, condition)

    def push(i, src, dst):
        return rcopy(src, dst, w_s.at[i], w_r.at[i], core)

    pushes = [
        push(0, eg_hbm.at[0], eg_o),
        push(1, sg_hbm, sg_o),
        push(2, su_hbm, su_o),
        push(3, sd_hbm, sd_o),
        push(4, eu_hbm.at[0], eu_o),
        push(5, ed_hbm.at[0], ed_o),
    ]
    for copy in pushes[:2]:
        copy.start()

    for k in range(2, 6):
        loads[k].wait()
    for load in loads[early:]:
        load.start()
    half = LANES // 2
    lane = lax.broadcasted_iota(jnp.int32, (rows, LANES), 1)
    unit = lax.broadcasted_iota(jnp.int32, (LANES, rows), 0)
    unit = jnp.where(unit < half, unit, unit - half)
    combine = jnp.zeros((LANES, rows), jnp.float32)
    for k in range(TOPK):
        combine = combine + jnp.where(routes_v[k : k + 1] == unit, gw_v[k : k + 1], 0.0)
    combine = combine.T
    high = combine.astype(jnp.bfloat16)
    low = (combine - high.astype(jnp.float32)).astype(jnp.bfloat16)
    own_tail = jnp.where(
        lane < half, high.astype(jnp.float32), low.astype(jnp.float32)
    ).astype(jnp.bfloat16)
    nrm[z, x, :, width:] = own_tail
    tail_s[...] = own_tail
    tail_copy = rcopy(tail_s, tail_m, slot(), w_r.at[6], xnbr)
    tail_copy.start()
    sent(tail_copy)

    contract = (((1,), (1,)), ((), ()))
    scale = HEAD ** (-0.5)

    def cols(head):
        return slice(head * HEAD, (head + 1) * HEAD)

    def stacked(kv):
        first = kv * grouped
        return jnp.concatenate(
            [q_v[:, cols(first + i)] for i in range(grouped)], axis=0
        ) * jnp.asarray(scale, q_v.dtype)

    def product(a, b):
        return lax.dot_general(a, b, contract, preferred_element_type=jnp.float32)

    queries = [stacked(kv) for kv in range(kv_heads)]
    row = lax.broadcasted_iota(jnp.int32, (grouped * length, 1), 0)
    tops = []
    sums = []
    outs = []
    for kv in range(kv_heads):
        scores = product(queries[kv], k_v[:, cols(kv)])
        sink = jnp.full((grouped * length, 1), sink_s[kv * grouped], jnp.float32)
        for i in range(1, grouped):
            sink = jnp.where(row >= i * length, sink_s[kv * grouped + i], sink)
        top = jnp.maximum(jnp.max(scores, axis=-1, keepdims=True), sink)
        e = jnp.exp(scores - top)
        tops.append(top)
        sums.append(jnp.exp(sink - top) + jnp.sum(e, axis=-1, keepdims=True))
        outs.append(
            jnp.dot(e.astype(jnp.bfloat16), v_v[:, cols(kv)], preferred_element_type=jnp.float32)
        )

    qi = lax.broadcasted_iota(jnp.int32, (grouped * length, length), 0) % length
    ki = lax.broadcasted_iota(jnp.int32, (grouped * length, length), 1)
    low_bound = jnp.where(z > 0, 0, length)
    high_bound = jnp.where(z < sp - 1, 0, length)
    low_mask = ki - qi >= low_bound
    high_mask = qi - ki >= high_bound

    def wait_halo(which):
        @pl.when(z > 0)
        def _():
            halo_wait(0, which)

        @pl.when(z < sp - 1)
        def _():
            halo_wait(1, which)

    wait_halo(0)
    sides = []
    for kv in range(kv_heads):
        s_low = jnp.where(low_mask, product(queries[kv], halo_k[0, :, cols(kv)]), -jnp.inf)
        s_high = jnp.where(high_mask, product(queries[kv], halo_k[1, :, cols(kv)]), -jnp.inf)
        top = jnp.max(jnp.maximum(s_low, s_high), axis=-1, keepdims=True)
        top = jnp.maximum(top, tops[kv])
        e_low = jnp.exp(s_low - top)
        e_high = jnp.exp(s_high - top)
        shrink = jnp.exp(tops[kv] - top)
        denominator = shrink * sums[kv] + jnp.sum(e_low + e_high, axis=-1, keepdims=True)
        sides.append(
            (
                shrink * outs[kv],
                e_low.astype(jnp.bfloat16),
                e_high.astype(jnp.bfloat16),
                1.0 / denominator,
            )
        )
    wait_halo(1)
    for kv in range(kv_heads):
        base, e_low, e_high, inverse = sides[kv]
        base = base + jnp.dot(
            e_low, halo_v[0, :, cols(kv)], preferred_element_type=jnp.float32
        )
        base = base + jnp.dot(
            e_high, halo_v[1, :, cols(kv)], preferred_element_type=jnp.float32
        )
        base = (base * inverse).astype(jnp.bfloat16)
        for i in range(grouped):
            att_v[:, :, cols(kv * grouped + i)] = base[i * length : (i + 1) * length].reshape(
                tp, rows, HEAD
            )

    @pl.when(z == 1)
    def _():
        signal(far_sem, at_z(z - 1))

    @pl.when(z == sp - 2)
    def _():
        signal(far_sem, at_z(z + 1))

    loads[6].wait()

    def projected(cc):
        picked = jnp.concatenate([att_v[xh * PAIR + cc] for xh in range(PAIR)], axis=0)
        return jnp.dot(picked, wo_v[...], preferred_element_type=jnp.float32)

    psend[...] = projected(1 - c).astype(jnp.bfloat16).reshape(psend.shape)
    pcore = []
    for order, xx in enumerate((1 - x, x)):
        pcore.append(rcopy(psend.at[xx], precv.at[xx], slot(), pr_sem.at[order], core))
        pcore[-1].start()
        sent(pcore[-1])
    for copy in pushes[2:]:
        copy.start()
    proj[...] = projected(c).reshape(proj.shape)
    piece = rows // CHUNKS

    def cut(j):
        return pl.ds(j * piece, piece)

    def cross(src, dst, k):
        copy = rcopy(src, dst, slot(), pr_sem.at[PAIR + k], xnbr)
        copy.start()
        sent(copy)
        return copy

    pcore[0].wait_recv()
    mirror_v[...] = proj[1 - x] + precv[1 - x].astype(jnp.float32)
    pcross = []
    for j in range(CHUNKS):
        pxs[cut(j)] = mirror_v[cut(j)].astype(jnp.bfloat16)
        pcross.append(cross(pxs.at[cut(j)], pxr.at[cut(j)], j))
    loads[7].wait()
    loads[8].wait()
    pcore[1].wait_recv()
    stream_v[...] = res_v[...].astype(jnp.float32) + proj[x] + precv[x].astype(jnp.float32)
    pmirror = []
    for j in range(CHUNKS):
        pys[cut(j)] = stream_v[cut(j)].astype(jnp.bfloat16)
        pmirror.append(cross(pys.at[cut(j)], pyr.at[cut(j)], CHUNKS + j))
    tail_copy.wait_recv()
    nrm[z, 1 - x, :, width:] = tail_m[...]

    def normalized(stream):
        return (
            stream
            * lax.rsqrt(jnp.mean(stream * stream, axis=-1, keepdims=True) + norm_eps)
            * gain_v[...]
        ).astype(jnp.bfloat16)

    expert = z * tp + t
    sibling = z * tp + t_core

    def schedule(me):
        def place(p):
            return p + upper * (sp - 1 - 2 * p)

        def send(src, dst, rsem, dev):
            copy = rcopy(src, dst, slot(), rsem, dev)
            copy.start()
            sent(copy)

        def side(h):
            return x if h == "o" else 1 - x

        def block_send(p, h, j, dev):
            g = place(p)
            ref = nrm.at[g, side(h), cut(j)]
            send(ref, ref, nrm_r.at[g, side(h), j], dev)

        def block_wait(p, h, j):
            g = place(p)
            ref = nrm.at[g, side(h), cut(j)]
            rcopy(ref, ref, send_sem.at[0], nrm_r.at[g, side(h), j], core).wait_recv()

        def cross_copy(p, j, sem):
            g = place(p)
            return rcopy(
                xsend.at[g, cut(j)], xrecv.at[g, cut(j)], sem, xr_sem.at[g, j], xnbr
            )

        lane_of = {"o": 0, "m": 1}

        def line_send(p, h, span):
            g = place(p)
            send(
                zsend.at[g, side(h), span],
                zrecv.at[z, side(h), span],
                zr_sem.at[z, lane_of[h]],
                at_z(g),
            )

        def line_wait(p, h):
            g = place(p)
            ref = zrecv.at[g, side(h)]
            rcopy(ref, ref, send_sem.at[0], zr_sem.at[g, lane_of[h]], core).wait_recv()
            return zrecv[g, side(h)].astype(jnp.float32)

        def add_send(p, j, adder):
            g = place(p)
            send(
                zsend.at[g, x, cut(j)], zadd.at[g, cut(j)], za_sem.at[g, j], at_z(place(adder))
            )

        def add_wait(p, j):
            g = place(p)
            ref = zadd.at[g, cut(j)]
            rcopy(ref, ref, send_sem.at[0], za_sem.at[g, j], core).wait_recv()
            return zadd[g, cut(j)].astype(jnp.float32)

        def cross_wait(p, j):
            cross_copy(p, j, send_sem.at[0]).wait_recv()
            g = place(p)
            return part[g, x, cut(j)] + xrecv[g, cut(j)].astype(jnp.float32)

        waited = set()

        def once(name, copies):
            if name not in waited:
                waited.add(name)
                for copy in copies:
                    copy()

        def own_weights():
            once("own", [loads[k].wait for k in range(9, 15)])

        def sibling_experts():
            once("experts", [pushes[k].wait_recv for k in (0, 4, 5)])

        def sibling_shared():
            once("shared", [pushes[k].wait_recv for k in (1, 2, 3)])

        def one(acts, gate_ref, up_ref, down_ref):
            gate = jnp.dot(acts, gate_ref[...], preferred_element_type=jnp.float32)
            up = jnp.dot(acts, up_ref[...], preferred_element_type=jnp.float32)
            hidden = (silu(gate) * up).astype(jnp.bfloat16)
            out = jnp.dot(hidden, down_ref[...], preferred_element_type=jnp.float32)
            return out.astype(jnp.bfloat16).astype(jnp.float32)

        def rows_of(places):
            block = [nrm[g].reshape(PAIR * rows, nrm.shape[-1]) for g in places]
            block = jnp.concatenate(block * 2 if len(block) == 1 else block, axis=0)
            return block[:, :width], block[:, width:].astype(jnp.float32)

        def weight(tail, e):
            lanes = lax.broadcasted_iota(jnp.int32, tail.shape, 1)
            mine = (lanes == e) | (lanes == e + half)
            return jnp.sum(jnp.where(mine, tail, 0.0), axis=-1, keepdims=True)

        def experts(ps):
            own_weights()
            sibling_experts()
            places = [place(p) for p in ps]
            acts, tail = rows_of(places)
            result = weight(tail, expert) * one(acts, eg_v, eu_v, ed_v)
            result = result + weight(tail, sibling) * one(acts, eg_o, eu_o, ed_o)
            result = result[: len(ps) * PAIR * rows].reshape(len(ps), PAIR, rows, width)
            for i, g in enumerate(places):
                part[g] = result[i]

        own_parts = [op for op in ORDER[me] if op[0] == "Q"]

        def own_part(op):
            own_weights()
            acts, tail = rows_of([z])
            if op[1] == 0:
                result = weight(tail, expert) * one(acts, eg_v, eu_v, ed_v)
            elif op[1] == 1:
                sibling_experts()
                result = weight(tail, sibling) * one(acts, eg_o, eu_o, ed_o)
            else:
                sibling_shared()
                result = one(acts, sg_v, su_v, sd_v) + one(acts, sg_o, su_o, sd_o)
            result = result[: PAIR * rows].reshape(PAIR, rows, width)
            if op == own_parts[0]:
                part[z] = result
            else:
                part[z] = part[z] + result

        knows_far = False
        summed = set()
        tail_from = None
        for op in ORDER[me]:
            kind = op[0]
            if kind == "E" and tail_from is None:
                tail_from = len(pending)
            if kind in "HG" and tail_from is not None and not summed:
                for index in range(tail_from):
                    settle(index)
                for copy in pushes:
                    copy.wait_send()
                summed.add(me)
            with jax.named_scope("op_" + "_".join(str(v) for v in op)):
                if kind == "N":
                    j = op[1]
                    pcross[j].wait_recv()
                    stream = stream_v[cut(j)] + pxr[cut(j)].astype(jnp.float32)
                    stream_v[cut(j)] = stream
                    nrm[z, x, cut(j), :width] = normalized(stream)
                elif kind == "M":
                    j = op[1]
                    pmirror[j].wait_recv()
                    stream = mirror_v[cut(j)] + pyr[cut(j)].astype(jnp.float32)
                    nrm[z, 1 - x, cut(j), :width] = normalized(stream)
                elif kind == "S":
                    h, p, j = op[1:]
                    if relay_of(me, p) is None and (
                        h == "o" or listed(me, p, DISPATCH_BY_LINE)
                    ):
                        if me == 0 and p == LINE - 1 and not knows_far:
                            pl.semaphore_wait(far_sem, 1)
                            knows_far = True
                        block_send(me, h, j, at_z(place(p)))
                elif kind == "A":
                    p, h, j = op[1:]
                    block_wait(p, h, j)
                    mirrored_in = listed(p, me, DISPATCH_BY_LINE)
                    if h == "o" and not mirrored_in:
                        block_send(p, h, j, xnbr)
                    for q in range(LINE):
                        if q not in (p, me) and relay_of(p, q) == me:
                            if h == "o" or (mirrored_in and listed(p, q, DISPATCH_BY_LINE)):
                                block_send(p, h, j, at_z(place(q)))
                elif kind == "D":
                    experts(op[1])
                elif kind == "Q":
                    own_part(op)
                elif kind == "E":
                    p = op[1]
                    g = place(p)
                    if p != me and listed(me, p, RETURN_BY_LINE):
                        for h in ("o", "m"):
                            zsend[g, side(h)] = part[g, side(h)].astype(jnp.bfloat16)
                            line_send(p, h, slice(None))
                    else:
                        if p == me:
                            for q in range(LINE):
                                if q != me and listed(q, me, RETURN_BY_LINE):
                                    part[g, 1 - x] = part[g, 1 - x] + line_wait(q, "m")
                        for j in range(CHUNKS):
                            xsend[g, cut(j)] = part[g, 1 - x, cut(j)].astype(jnp.bfloat16)
                            copy = cross_copy(p, j, slot())
                            copy.start()
                            sent(copy)
                elif kind == "F":
                    p, j = op[1:]
                    if not listed(me, p, RETURN_BY_LINE):
                        value = cross_wait(p, j)
                        for q in range(LINE):
                            if q not in (p, me) and adder_of(q, p) == me:
                                value = value + add_wait(p, j)
                        zsend[place(p), x, cut(j)] = value.astype(jnp.bfloat16)
                        adder = adder_of(me, p)
                        if adder is None:
                            line_send(p, "o", cut(j))
                        else:
                            add_send(p, j, adder)
                elif kind == "H":
                    j = op[1]
                    stream_v[cut(j)] = stream_v[cut(j)] + cross_wait(me, j)
                elif kind == "G":
                    p = op[1]
                    last = [other for other in ORDER[me] if other[:2] == ("G", p)][-1]
                    if op == last and adder_of(p, me) is None:
                        stream_v[...] = stream_v[...] + line_wait(p, "o")
        out_ref[...] = stream_v[...].astype(out_ref.dtype)
        if me == 0 and not knows_far:
            pl.semaphore_wait(far_sem, 1)
        with jax.named_scope("lastwaits"):
            for index in range(len(pending)):
                settle(index)

    shared_pending = list(pending)
    for me in range(LINE // 2):

        @pl.when((z == me) | (z == sp - 1 - me))
        def _():
            pending[:] = shared_pending
            schedule(me)


def fused_scratch(sp, tp, shapes):
    (q, k, v, sink, wo, res, gain, routes, gw, eg, eu, ed, sg, su, sd) = shapes
    rows, width = res.shape
    bf = jnp.bfloat16
    f32 = jnp.float32
    return [
        (q.shape, bf),
        (k.shape, bf),
        (v.shape, bf),
        (sink.shape, f32),
        (wo.shape, bf),
        (res.shape, bf),
        (gain.shape, f32),
        (routes.shape, jnp.int32),
        (gw.shape, f32),
        (eg.shape[1:], bf),
        (eu.shape[1:], bf),
        (ed.shape[1:], bf),
        (sg.shape, bf),
        (su.shape, bf),
        (sd.shape, bf),
        (eg.shape[1:], bf),
        (eu.shape[1:], bf),
        (ed.shape[1:], bf),
        (sg.shape, bf),
        (su.shape, bf),
        (sd.shape, bf),
        ((2,) + k.shape, bf),
        ((2,) + v.shape, bf),
        ((tp, rows, q.shape[1]), bf),
        ((PAIR, rows, width), f32),
        ((PAIR, rows, width), bf),
        ((PAIR, rows, width), bf),
        ((rows, width), bf),
        ((rows, width), bf),
        ((rows, width), bf),
        ((rows, width), bf),
        ((rows, width), f32),
        ((rows, width), f32),
        ((rows, LANES), bf),
        ((rows, LANES), bf),
        ((sp, PAIR, rows, width + LANES), bf),
        ((sp, PAIR, rows, width), f32),
        ((sp, rows, width), bf),
        ((sp, rows, width), bf),
        ((sp, PAIR, rows, width), bf),
        ((sp, PAIR, rows, width), bf),
        ((sp, rows, width), bf),
    ]


def size_of(shape, dtype):
    total = jnp.dtype(dtype).itemsize
    for extent in shape:
        total *= extent
    return total


def fused(sp, tp, buffers, *args):
    dma = pltpu.SemaphoreType.DMA
    res = args[5]
    scratch = [pltpu.VMEM(s, d) for s, d in buffers]
    scratch[3] = pltpu.SMEM(*buffers[3])
    return pl.pallas_call(
        functools.partial(fused_kernel, sp, tp),
        out_shape=pltpu.VMEM(res.shape, jnp.bfloat16),
        in_specs=[pl.BlockSpec(memory_space=pltpu.HBM)] * 15,
        out_specs=pl.BlockSpec(memory_space=pltpu.VMEM),
        scratch_shapes=scratch
        + [
            dma((9,)),
            dma((2, 2)),
            dma((PAIR + 2 * CHUNKS,)),
            dma((6,)),
            dma((7,)),
            dma((SENDS,)),
            dma((sp, PAIR, CHUNKS)),
            dma((sp, CHUNKS)),
            dma((sp, PAIR)),
            dma((sp, CHUNKS)),
            pltpu.SemaphoreType.REGULAR,
        ],
        compiler_params=pltpu.CompilerParams(
            collective_id=0, has_side_effects=True, vmem_limit_bytes=VMEM_BYTES
        ),
    )(*args)


def either(*args):
    sp = lax.axis_size("sp")
    tp = lax.axis_size("tp")
    args = list(args)
    shaped = list(args)
    shaped[6] = args[6].reshape(1, -1)
    shaped[7] = args[7].T
    shaped[8] = args[8].T
    buffers = fused_scratch(sp, tp, shaped)
    needed = sum(size_of(s, d) for s, d in buffers)
    fits = (
        2 * needed <= VMEM_BYTES
        and tp == 2 * PAIR
        and sp == LINE
        and args[5].shape[0] % (16 * CHUNKS) == 0
        and 2 * sp * tp <= LANES
        and args[0].shape[0] == WINDOW
        and args[9].shape[0] == 1
    )
    if fits:
        return fused(sp, tp, buffers, *shaped)
    return body(*args)


def solution(mesh):
    placed = (
        P(("grp", "sp"), "tp"),
        P(("grp", "sp"), "tp"),
        P(("grp", "sp"), "tp"),
        P("tp"),
        P("tp", None),
        P(("grp", "sp", "tp"), None),
        P(),
        P(("grp", "sp", "tp"), None),
        P(("grp", "sp", "tp"), None),
        P(("sp", "tp"), None, None),
        P(("sp", "tp"), None, None),
        P(("sp", "tp"), None, None),
        P(None, "tp"),
        P(None, "tp"),
        P("tp", None),
    )
    return jax.shard_map(
        either, mesh=mesh, in_specs=placed, out_specs=P(("grp", "sp", "tp"), None), check_vma=False
    )
```
